256 devices in a mesh: grp: 2 (over y), ep: 32 (over z, core), tp: 4 (over x).
Axes of the slice: x: 4, y: 2, z: 16, core: 2. Of those that a mesh axis runs over, the one named last changes fastest.
The devices are a block of a 4x16x16 slice.
Arguments:
- queries: bfloat16 [32768, 1024], P(('grp', 'ep'), 'tp'), parts along dimension 0, may hold values from -6 to 6
- key_rows: bfloat16 [32768, 512], P(('grp', 'ep'), 'tp'), parts along dimension 0, may hold values from -6 to 6
- value_rows: bfloat16 [32768, 512], P(('grp', 'ep'), 'tp'), parts along dimension 0, may hold values from -6 to 6
- query_gain: float32 [128], replicated, may hold values from 0.3 to 9
- key_gain: float32 [128], replicated, may hold values from 0.3 to 9
- log_forget: float32 [8, 32768], P('tp', 'grp'), parts along dimension 1, may hold values from -16384 to 0, as said below
- out_weight: bfloat16 [1024, 2048], P('tp'), may hold values from -0.1875 to 0.1875
- expert_rows: bfloat16 [32768, 2048], P(('grp', 'ep')), parts along dimension 0, may hold values from -6 to 6
- expert_gain: float32 [2048], replicated, may hold values from 0.1 to 1.9
- routes: int32 [2, 32768], P(None, ('grp', 'ep')), parts along dimension 1, may hold values from 0 to 31, as said below
- route_weight: float32 [2, 32768], P(None, ('grp', 'ep')), parts along dimension 1, may hold values from 0.1 to 1
- gate_weight: bfloat16 [32, 2048, 1024], P('ep', None, 'tp'), may hold values from -0.125 to 0.125
- up_weight: bfloat16 [32, 2048, 1024], P('ep', None, 'tp'), may hold values from -0.125 to 0.125
- down_weight: bfloat16 [32, 1024, 2048], P('ep', 'tp'), may hold values from -0.1875 to 0.1875
Outputs:
- mixer_out: bfloat16 [32768, 2048], P(('grp', 'ep', 'tp')), parts along dimension 0
- expert_out: bfloat16 [32768, 2048], P(('grp', 'ep'), 'tp'), parts along dimension 0
The draws below stay inside these ranges and needn't reach their ends.
There are 2 independent parts, one for each index of `grp`. The reference program is written for one: setup_inputs(seed, part) draws one part's arguments, and reference() takes and returns one part's arrays. A program takes and returns all parts, laid end to end along the dimension named above; an argument that names none is the same for every part. Nothing has to cross between parts.
Inputs may be any that keep to these rules, and one draw needn't show every extreme that they name: `log_forget`: each head's values never rise along the positions. `routes`: the 2 experts of a token differ and lie in one group of 8 consecutive numbers. Among the tokens of one index of ep (512 consecutive tokens), no expert is named more than 48 times, and in every draw some experts are named exactly 48 times in every such block.
All inputs are finite; a program needn't handle non-finite values.
Results may differ from the reference program's by a relative error of at most 0.012.
The reference program's roundings to bfloat16 on the way count: a program that leaves them out, or rounds other values in their place, can miss the bound.
Values may be sent and summed in bfloat16 or wider, within the bound.
A program may use at most 128 MiB of HBM per device.

```python
import math
import jax
import jax.numpy as jnp
from jax import lax

D = 2048
QUERY_HEADS = 8
KV_HEADS = 4
HEAD_SIZE = 128
EXPERTS = 32
GROUP_SIZE = 8
FF = 1024
TOP = 2
SPAN = 512
SEQUENCE_TOKENS = 16384
CAP = 48
N_EP = 32
N_TP = 4


def gain_draw(gain_key):
    return jnp.clip(1.0 + 0.18 * jax.random.normal(gain_key, (HEAD_SIZE,), jnp.float32), 0.3, 1.7)


def draw_query_gain(key, part):
    return gain_draw(jax.random.fold_in(key, 3))


def draw_key_gain(key, part):
    return gain_draw(jax.random.fold_in(key, 5))


def draw_log_forget(key, part):
    divided_keys = jax.random.split(jax.random.fold_in(key, 7), 7)
    token_position = jnp.arange(SEQUENCE_TOKENS, dtype=jnp.int32)
    shard_factor = jnp.exp(jax.random.uniform(divided_keys[0], (SEQUENCE_TOKENS // SPAN,), jnp.float32, -0.7, 0.7))
    factor_vector = jnp.repeat(shard_factor, SPAN)
    fast_rank = jax.random.permutation(divided_keys[1], QUERY_HEADS).astype(jnp.int32)
    is_fast = fast_rank < QUERY_HEADS // 2
    slow_rate = jax.random.uniform(divided_keys[2], (QUERY_HEADS,), jnp.float32, 0.3, 0.9) / SEQUENCE_TOKENS
    fast_rate = 1.0 / jax.random.uniform(divided_keys[3], (QUERY_HEADS,), jnp.float32, 30.0, 50.0)
    baseline_rate = jnp.where(is_fast, fast_rate, slow_rate)
    jitter_amount = jax.random.uniform(divided_keys[4], (QUERY_HEADS, SEQUENCE_TOKENS), jnp.float32, 0.5, 1.5)
    spike_position = jax.random.randint(divided_keys[5], (QUERY_HEADS, 3), 0, SEQUENCE_TOKENS)
    spike_length = -jnp.log(jax.random.uniform(divided_keys[6], (QUERY_HEADS, 3), jnp.float32, 0.6, 0.8))
    spike_events = jnp.sum(jnp.where(token_position[None, None, :] == spike_position[:, :, None], spike_length[:, :, None], 0.0), axis=1)
    logarithm_step = -(baseline_rate[:, None] * factor_vector[None, :] * jitter_amount + spike_events)
    return jnp.cumsum(logarithm_step, axis=1)


def route_block(block_key, full_group):
    divided_keys = jax.random.split(block_key, 4)
    full_rows = GROUP_SIZE * CAP // 2
    rest_rows = SPAN - full_rows
    other_sizes = jnp.array([rest_rows // 2, rest_rows // 3, rest_rows - rest_rows // 2 - rest_rows // 3], jnp.int32)
    others = (full_group + 1 + jax.random.permutation(divided_keys[0], 3).astype(jnp.int32)) % 4
    group_sizes = jnp.zeros((4,), jnp.int32).at[full_group].set(full_rows).at[others].set(other_sizes)
    group_ends = jnp.cumsum(group_sizes)
    token_position = jnp.arange(SPAN, dtype=jnp.int32)
    group_of = jnp.sum((token_position[:, None] >= group_ends[None, :]).astype(jnp.int32), axis=1)
    within = token_position - (group_ends - group_sizes)[group_of]
    orders = jax.vmap(lambda sub_key: jax.random.permutation(sub_key, GROUP_SIZE).astype(jnp.int32))(jax.random.split(divided_keys[1], 4))
    shifts = jax.random.randint(divided_keys[2], (4,), 0, GROUP_SIZE - 1)
    first_pick = orders[group_of, within % GROUP_SIZE]
    second_pick = orders[group_of, (within + 1 + (within // GROUP_SIZE + shifts[group_of]) % (GROUP_SIZE - 1)) % GROUP_SIZE]
    chosen = jnp.stack([group_of * GROUP_SIZE + first_pick, group_of * GROUP_SIZE + second_pick])
    shuffle = jax.random.permutation(divided_keys[3], SPAN)
    return chosen[:, shuffle]


def draw_routes(key, part):
    full_group = jax.random.randint(jax.random.fold_in(key, 11), (), 0, 4)
    block_keys = jax.random.split(jax.random.fold_in(key, 12), SEQUENCE_TOKENS // SPAN)
    blocks = jax.vmap(lambda block_key: route_block(block_key, full_group))(block_keys)
    return jnp.transpose(blocks, (1, 0, 2)).reshape(2, SEQUENCE_TOKENS).astype(jnp.int32)


def steps_of(key, dims, cuts, smallest, high):
    def one(position, parts):
        draws = jax.random.uniform(jax.random.fold_in(jax.random.fold_in(key, 6), position), (parts,), jnp.float32, smallest / len(cuts), high / len(cuts))
        return jnp.repeat(jnp.exp(draws), dims[position] // parts).reshape((-1,) + (1,) * (len(dims) - position - 1))

    factor_of = one(*cuts[0])
    for cut in cuts[1:]:
        factor_of = factor_of * one(*cut)
    return factor_of


def noise(rng, shape, spread, bound, cuts=(), held_as=jnp.bfloat16):
    result = jax.random.normal(rng, shape, jnp.float32) * spread
    if len(cuts) > 0:
        result = steps_of(rng, shape, cuts, -0.22, 0.18) * result
    return jnp.clip(result, min=-bound, max=bound).astype(held_as)


def setup_inputs(seed: int = 0, part: int = 0) -> dict:
    keys = jax.random.split(jax.random.key(seed), 15)
    part_keys = jax.random.split(jax.random.fold_in(keys[14], part), 15)
    return {
        "queries": noise(part_keys[0], (SEQUENCE_TOKENS, QUERY_HEADS * HEAD_SIZE), 1.0, 6.0, ((0, 32), (1, 4))),
        "key_rows": noise(part_keys[1], (SEQUENCE_TOKENS, KV_HEADS * HEAD_SIZE), 1.0, 6.0, ((0, 32), (1, 4))),
        "value_rows": noise(part_keys[2], (SEQUENCE_TOKENS, KV_HEADS * HEAD_SIZE), 1.0, 6.0, ((0, 32), (1, 4))),
        "query_gain": draw_query_gain(jax.random.fold_in(keys[14], 71), part),
        "key_gain": draw_key_gain(jax.random.fold_in(keys[14], 71), part),
        "log_forget": draw_log_forget(jax.random.fold_in(jax.random.fold_in(keys[14], part), 71), part),
        "out_weight": noise(keys[6], (QUERY_HEADS * HEAD_SIZE, D), (QUERY_HEADS * HEAD_SIZE) ** -0.5, 0.1875, ((0, 4),)),
        "expert_rows": noise(part_keys[7], (SEQUENCE_TOKENS, D), 1.0, 6.0, ((0, 32),)),
        "expert_gain": jnp.clip(1.0 + 0.18 * jax.random.normal(keys[8], (D,), jnp.float32), 0.1, 1.9),
        "routes": draw_routes(jax.random.fold_in(jax.random.fold_in(keys[14], part), 71), part),
        "route_weight": jnp.clip(jnp.exp(math.log(1.0) - 2.3025851 * jax.random.uniform(part_keys[10], (TOP, SEQUENCE_TOKENS), jnp.float32) ** steps_of(part_keys[10], (TOP, SEQUENCE_TOKENS), ((1, 32),), -0.2, 0.2)), 0.1, 1.0),
        "gate_weight": noise(keys[11], (EXPERTS, D, FF), D ** -0.5, 0.125, ((0, 32), (2, 4))),
        "up_weight": noise(keys[12], (EXPERTS, D, FF), D ** -0.5, 0.125, ((0, 32), (2, 4))),
        "down_weight": noise(keys[13], (EXPERTS, FF, D), FF ** -0.5, 0.1875, ((0, 32), (1, 4))),
    }


def head_norm(inputs, scale_gain):
    widened = inputs.astype(jnp.float32)
    factor = lax.rsqrt(lax.optimization_barrier(jnp.mean(widened * widened, axis=-1, keepdims=True)) + 1e-06)
    return widened * factor * scale_gain.astype(jnp.float32)

def slot_table(chosen, experts_all, capacity):
    n_rows = chosen.shape[0]
    per_row = chosen.shape[1]
    flat_ids = chosen.reshape(-1)
    one_hot = (flat_ids[:, None] == jnp.arange(experts_all, dtype=jnp.int32)[None, :]).astype(jnp.int32)
    within = lax.optimization_barrier(jnp.sum((jnp.cumsum(one_hot, axis=0) - 1) * one_hot, axis=1))
    slot_index = (flat_ids * capacity + within).astype(jnp.int32)
    row_of = jnp.arange(n_rows * per_row, dtype=jnp.int32) // per_row
    slot_owner = jnp.full((experts_all * capacity,), n_rows, jnp.int32).at[slot_index].set(row_of)
    return (slot_index.reshape(n_rows, per_row), slot_owner)

def reference(queries, key_rows, value_rows, query_gain, key_gain, log_forget, out_weight, expert_rows, expert_gain, routes, route_weight, gate_weight, up_weight, down_weight):
    span_len = SEQUENCE_TOKENS // N_EP
    group_ratio = QUERY_HEADS // KV_HEADS
    scale_qk = HEAD_SIZE ** (-0.5)
    q_all = lax.optimization_barrier(head_norm(queries.reshape(SEQUENCE_TOKENS, KV_HEADS, group_ratio, HEAD_SIZE), query_gain).astype(jnp.bfloat16)).astype(jnp.float32)
    k_all = lax.optimization_barrier(head_norm(key_rows.reshape(SEQUENCE_TOKENS, KV_HEADS, HEAD_SIZE), key_gain).astype(jnp.bfloat16)).astype(jnp.float32)
    v_all = value_rows.reshape(SEQUENCE_TOKENS, KV_HEADS, HEAD_SIZE).astype(jnp.float32)
    positions = jnp.arange(span_len, dtype=jnp.int32)

    def query_block(block_index):
        q_here = lax.dynamic_slice_in_dim(q_all, block_index * span_len, span_len, 0)
        gates_here = lax.dynamic_slice_in_dim(log_forget, block_index * span_len, span_len, 1)
        gates_here = gates_here.T.reshape(span_len, KV_HEADS, group_ratio)

        def key_step(key_index, running):
            run_max, run_sum, run_acc = running
            k_here = lax.dynamic_slice_in_dim(k_all, key_index * span_len, span_len, 0)
            v_here = lax.dynamic_slice_in_dim(v_all, key_index * span_len, span_len, 0)
            key_gates = lax.dynamic_slice_in_dim(log_forget, key_index * span_len, span_len, 1)
            key_gates = key_gates.reshape(KV_HEADS, group_ratio, span_len)
            scores = jnp.einsum('qgrd,kgd->qgrk', q_here, k_here) * scale_qk
            scores = scores + gates_here[..., None] - key_gates[None]
            visible = (key_index * span_len + positions)[None, :] <= (block_index * span_len + positions)[:, None]
            scores = jnp.where(visible[:, None, None, :], scores, -jnp.inf)
            new_max = jnp.maximum(run_max, lax.optimization_barrier(jnp.max(scores, axis=-1)))
            shrink = jnp.exp(run_max - new_max)
            weights = jnp.exp(scores - new_max[..., None])
            run_sum = shrink * run_sum + lax.optimization_barrier(jnp.sum(weights, axis=-1))
            weights_low = lax.optimization_barrier(weights.astype(jnp.bfloat16)).astype(jnp.float32)
            gathered = jnp.einsum('qgrk,kgd->qgrd', weights_low, v_here)
            return (new_max, run_sum, shrink[..., None] * run_acc + gathered)
        start_state = (jnp.full((span_len, KV_HEADS, group_ratio), -jnp.inf, jnp.float32), jnp.zeros((span_len, KV_HEADS, group_ratio), jnp.float32), jnp.zeros((span_len, KV_HEADS, group_ratio, HEAD_SIZE), jnp.float32))
        run_max, run_sum, run_acc = lax.fori_loop(0, block_index + 1, key_step, start_state)
        return (run_acc / run_sum[..., None]).astype(jnp.bfloat16)
    attended = lax.map(query_block, jnp.arange(N_EP, dtype=jnp.int32))
    attended = attended.reshape(SEQUENCE_TOKENS, QUERY_HEADS * HEAD_SIZE)
    mixer_out = jnp.dot(attended, out_weight, preferred_element_type=jnp.float32).astype(jnp.bfloat16)
    normed = head_norm(expert_rows, expert_gain).astype(jnp.bfloat16)
    block_routes = routes.reshape(TOP, N_EP, span_len).transpose(1, 2, 0)
    slot_all, owner_all = jax.vmap(lambda chosen: slot_table(chosen, EXPERTS, CAP))(block_routes)
    block_base = jnp.arange(N_EP, dtype=jnp.int32)[:, None] * span_len
    global_rows = jnp.where(owner_all == span_len, SEQUENCE_TOKENS, owner_all + block_base).astype(jnp.int32)
    row_index = global_rows.reshape(N_EP, EXPERTS, CAP).transpose(1, 0, 2).reshape(EXPERTS, N_EP * CAP)
    padded = jnp.concatenate([normed, jnp.zeros((1, D), jnp.bfloat16)], axis=0)
    ff_part = FF // N_TP

    def one_expert(inputs):
        index_rows, w_gate, w_up, w_down = inputs
        taken = padded[index_rows]
        gate_part = jnp.dot(taken, w_gate, preferred_element_type=jnp.float32)
        up_part = jnp.dot(taken, w_up, preferred_element_type=jnp.float32)
        hidden = (jax.nn.silu(gate_part) * up_part).astype(jnp.bfloat16)
        running = jnp.zeros((N_EP * CAP, D), jnp.float32)
        for part_index in range(N_TP):
            piece = jnp.dot(hidden[:, part_index * ff_part:(part_index + 1) * ff_part], w_down[part_index * ff_part:(part_index + 1) * ff_part], preferred_element_type=jnp.float32)
            running = running + lax.optimization_barrier(piece.astype(jnp.bfloat16)).astype(jnp.float32)
        return running.astype(jnp.bfloat16)
    results = lax.map(one_expert, (row_index, gate_weight, up_weight, down_weight))
    result_table = results.reshape(EXPERTS, N_EP, CAP, D)
    expert_of = slot_all // CAP
    cell_of = slot_all % CAP
    block_id = jnp.arange(N_EP, dtype=jnp.int32)[:, None, None]
    picked = result_table[expert_of, block_id, cell_of]
    weights_all = route_weight.reshape(TOP, N_EP, span_len).transpose(1, 2, 0)
    expert_out = lax.optimization_barrier(jnp.sum(picked.astype(jnp.float32) * weights_all[..., None], axis=2))
    expert_out = expert_out.astype(jnp.bfloat16).reshape(SEQUENCE_TOKENS, D)
    return (mixer_out, expert_out)
```

```python
import functools

import jax
import jax.numpy as jnp
from jax import lax
from jax.experimental import pallas as pl
from jax.experimental.pallas import tpu as pltpu
from jax.sharding import PartitionSpec as P

HEAD_SIZE = 128
EXPERTS = 32
CAP = 48
TOP = 2
CORES = 2
LOG2E = 1.4426950408889634
MESH = pl.DeviceIdType.MESH
F32 = jnp.float32
BF16 = jnp.bfloat16


def dot(a, b, dims=(((1,), (0,)), ((), ()))):
    return lax.dot_general(a, b, dims, preferred_element_type=F32)


def row_norm(rows, gain):
    wide = rows.astype(F32)
    factor = lax.rsqrt(jnp.mean(wide * wide, axis=-1, keepdims=True) + 1e-06)
    return wide * factor * gain


def member_and_rank(routes, expert_col):
    tokens = routes.shape[1]
    count = expert_col.shape[0]
    named = jnp.logical_or(routes[0:1, :] == expert_col, routes[1:2, :] == expert_col)
    member = jnp.where(named, 1.0, 0.0).astype(F32)
    before = lax.broadcasted_iota(jnp.int32, (tokens, tokens), 0)
    after = lax.broadcasted_iota(jnp.int32, (tokens, tokens), 1)
    earlier = jnp.where(before < after, 1.0, 0.0).astype(BF16)
    del count
    return member, dot(member.astype(BF16), earlier)


def prologue_kernel(
    n_tp, rows_ref, gain_ref, routes_ref, key_ref, value_ref, key_gain_ref, send_ref, kv_ref, normed
):
    span = rows_ref.shape[0]
    me, t = lax.axis_index("ep"), lax.axis_index("tp")
    offset = lax.rem(t + (n_tp - 1) * me, n_tp)
    kv_ref[:, :HEAD_SIZE] = row_norm(key_ref[...], key_gain_ref[...]).astype(BF16)
    kv_ref[:, HEAD_SIZE:] = value_ref[...]
    step = 64
    for first in range(0, span, step):
        normed[first : first + step, :] = row_norm(
            rows_ref[first : first + step, :], gain_ref[...]
        ).astype(BF16)
    here = EXPERTS // n_tp
    expert_col = offset + n_tp * lax.broadcasted_iota(jnp.int32, (here, 1), 0)
    member, rank = member_and_rank(routes_ref[...], expert_col)
    place = jnp.where(member > 0.5, rank, -1.0)
    slot = lax.broadcasted_iota(jnp.int32, (CAP, span), 0).astype(F32)
    for m in range(here):
        pick = jnp.where(place[m : m + 1, :] == slot, 1.0, 0.0).astype(BF16)
        send_ref[m] = dot(pick, normed[...]).astype(BF16)


def spread_kernel(
    n_ep,
    n_tp,
    send_ref,
    kv_ref,
    gate_ref,
    up_ref,
    down_ref,
    out_ref,
    recv_ref,
    kv_all,
    gate_all,
    up_all,
    down_all,
    out_all,
    row_send,
    row_recv,
    fwd_send,
    fwd_recv,
    bwd_send,
    bwd_recv,
    core_send,
    core_recv,
    side_send,
    side_recv,
    half_send,
    half_recv,
    local,
):
    me, t = lax.axis_index("ep"), lax.axis_index("tp")
    n_z = n_ep // CORES
    z, core = me // CORES, lax.rem(me, CORES)
    offset = lax.rem(t + (n_tp - 1) * me, n_tp)
    here = n_ep // n_tp
    right, left = lax.rem(t + 1, n_tp), lax.rem(t + n_tp - 1, n_tp)
    across = lax.rem(t + 2, n_tp)
    up_ep = CORES * lax.rem(z + 1, n_z) + core
    down_ep = CORES * lax.rem(z + n_z - 1, n_z) + core
    other = CORES * z + (1 - core)
    reach = n_z // 2
    self_slot = me // n_tp
    is_self = lax.rem(me, n_tp) == offset

    barrier = pltpu.get_barrier_semaphore()
    for where in (
        {"ep": up_ep},
        {"ep": down_ep},
        {"ep": other},
        {"tp": right},
        {"tp": left},
    ):
        pl.semaphore_signal(barrier, inc=1, device_id=where, device_id_type=MESH)
    for m in range(here):
        mate = offset + n_tp * m

        @pl.when(mate != me)
        def _():
            pl.semaphore_signal(barrier, inc=1, device_id={"ep": mate}, device_id_type=MESH)

    pl.semaphore_wait(barrier, 5 + here - jnp.where(is_self, 1, 0))

    def remote(src, dst, send_sem, recv_sem, where):
        return pltpu.make_async_remote_copy(
            src_ref=src,
            dst_ref=dst,
            send_sem=send_sem,
            recv_sem=recv_sem,
            device_id=where,
            device_id_type=MESH,
        )

    arrays = ((gate_ref, gate_all), (up_ref, up_all), (down_ref, down_all))
    out_rows = out_ref.shape[0] // CORES
    out_first = core * out_rows

    def side_copy(a, to_right):
        where = {"tp": right} if to_right else {"tp": left}
        way = 0 if to_right else 1
        if a < 3:
            src, dst = arrays[a][0], arrays[a][1].at[t]
        else:
            mine = pl.ds(out_first, out_rows)
            src, dst = out_ref.at[mine], out_all.at[t, mine]
        return remote(src, dst, side_send.at[a, way], side_recv.at[a, way], where)

    def half_copy(a, to_right):
        where = {"tp": right} if to_right else {"tp": left}
        way = 0 if to_right else 1
        owner = left if to_right else right
        if a < 3:
            full = arrays[a][1]
            half = full.shape[1] // 2
            part = full.at[owner, pl.ds(way * half, half)]
        else:
            half = out_rows // 2
            part = out_all.at[owner, pl.ds(out_first + way * half, half)]
        return remote(part, part, half_send.at[a, way], half_recv.at[a, way], where)

    def out_copy(k):
        owner = (left, right, across)[k]
        part = out_all.at[owner, pl.ds(out_first, out_rows)]
        return remote(part, part, core_send.at[k], core_recv.at[k], {"ep": other})

    def kv_copy(source_z, source_core, send_sem, recv_sem, where, own=False):
        block = kv_all.at[CORES * source_z + source_core]
        return remote(kv_ref if own else block, block, send_sem, recv_sem, where)

    def fwd_copy(s):
        return kv_copy(
            lax.rem(z - s + n_z, n_z), core, fwd_send.at[s], fwd_recv.at[s], {"ep": up_ep}, s == 0
        )

    def bwd_copy(s):
        return kv_copy(
            lax.rem(z + s, n_z), core, bwd_send.at[s], bwd_recv.at[s], {"ep": down_ep}, s == 0
        )

    def row_copy(k):
        m = lax.rem(self_slot + k, here)
        mate = offset + n_tp * m
        return mate, remote(
            send_ref.at[m],
            recv_ref.at[self_slot],
            row_send.at[m],
            row_recv.at[self_slot],
            {"ep": mate},
        )

    def row_local():
        return pltpu.make_async_copy(
            send_ref.at[self_slot], recv_ref.at[self_slot], local.at[5]
        )

    def fwd_sends(s):
        return jnp.logical_and(z - s >= 0, z + 1 <= n_z - 1)

    def fwd_gets(s):
        return z - 1 - s >= 0

    def bwd_sends(s):
        return lax.rem(z + s, n_z) <= reach - 2

    def bwd_gets(s):
        return lax.rem(z + 1 + s, n_z) <= reach - 2

    def bwd_needed(s):
        return jnp.logical_and(bwd_gets(s), lax.rem(z + 1 + s, n_z) < z)

    for a in range(4):
        side_copy(a, True).start()
        side_copy(a, False).start()
    own = [
        pltpu.make_async_copy(kv_ref, kv_all.at[me], local.at[0]),
        pltpu.make_async_copy(gate_ref, gate_all.at[t], local.at[1]),
        pltpu.make_async_copy(up_ref, up_all.at[t], local.at[2]),
        pltpu.make_async_copy(down_ref, down_all.at[t], local.at[3]),
        pltpu.make_async_copy(out_ref, out_all.at[t], local.at[4]),
    ]
    for copy in own:
        copy.start()

    @pl.when(is_self)
    def _():
        row_local().start()

    def core_own():
        return kv_copy(z, core, core_send.at[3], core_recv.at[3], {"ep": other}, True)

    def core_fwd(s, source_core):
        return kv_copy(
            lax.rem(z - 1 - s + n_z, n_z),
            source_core,
            core_send.at[4 + s],
            core_recv.at[4 + s],
            {"ep": other},
        )

    def core_bwd(s, source_core):
        return kv_copy(
            lax.rem(z + 1 + s, n_z),
            source_core,
            core_send.at[4 + reach + s],
            core_recv.at[4 + reach + s],
            {"ep": other},
        )

    @pl.when(core == 0)
    def _():
        core_own().start()

    for s in range(reach):
        if s > 0:

            @pl.when(fwd_gets(s - 1))
            def _():
                fwd_copy_in(kv_copy, kv_all, z, n_z, core, s - 1, fwd_send, fwd_recv, up_ep)
                core_fwd(s - 1, core).start()

        @pl.when(fwd_sends(s))
        def _():
            fwd_copy(s).start()

        if s < reach - 1:
            if s > 0:

                @pl.when(bwd_gets(s - 1))
                def _():
                    bwd_copy_in(kv_copy, z, n_z, core, s - 1, bwd_send, bwd_recv, down_ep)

                @pl.when(bwd_needed(s - 1))
                def _():
                    core_bwd(s - 1, core).start()

            @pl.when(bwd_sends(s))
            def _():
                bwd_copy(s).start()

        mate, copy = row_copy(s)

        @pl.when(mate != me)
        def _(copy=copy):
            copy.start()

        if s in (2, 4, 6):
            a = (2, 4, 6).index(s)
            side_copy(a, True).wait_recv()
            half_copy(a, True).start()
            side_copy(a, False).wait_recv()
            half_copy(a, False).start()

    last = reach - 1

    @pl.when(fwd_gets(last))
    def _():
        fwd_copy_in(kv_copy, kv_all, z, n_z, core, last, fwd_send, fwd_recv, up_ep)
        core_fwd(last, core).start()

    @pl.when(bwd_gets(last - 1))
    def _():
        bwd_copy_in(kv_copy, z, n_z, core, last - 1, bwd_send, bwd_recv, down_ep)

    @pl.when(bwd_needed(last - 1))
    def _():
        core_bwd(last - 1, core).start()

    side_copy(3, True).wait_recv()
    half_copy(3, True).start()
    side_copy(3, False).wait_recv()
    half_copy(3, False).start()
    out_copy(0).start()
    out_copy(1).start()
    half_copy(3, True).wait_recv()
    half_copy(3, False).wait_recv()
    out_copy(2).start()

    for a in range(4):
        for to_right in (True, False):
            side_copy(a, to_right).wait_send()
            if a < 3:
                half_copy(a, to_right).wait_recv()
            half_copy(a, to_right).wait_send()
    for k in range(here):
        mate, copy = row_copy(k)

        @pl.when(mate != me)
        def _(copy=copy):
            copy.wait_send()

        source = offset + n_tp * k
        arrival = remote(
            send_ref.at[k], recv_ref.at[k], row_send.at[k], row_recv.at[k], {"ep": source}
        )

        @pl.when(source != me)
        def _(arrival=arrival):
            arrival.wait_recv()

    for s in range(reach):

        @pl.when(fwd_sends(s))
        def _():
            fwd_copy(s).wait_send()

        @pl.when(fwd_gets(s))
        def _():
            core_fwd(s, core).wait_send()
            core_fwd(s, 1 - core).wait_recv()

        if s < reach - 1:

            @pl.when(bwd_sends(s))
            def _():
                bwd_copy(s).wait_send()

            @pl.when(bwd_needed(s))
            def _():
                core_bwd(s, core).wait_send()
                core_bwd(s, 1 - core).wait_recv()

    for k in range(3):
        out_copy(k).wait_send()
        out_first_other = (1 - core) * out_rows
        owner = (left, right, across)[k]
        part = out_all.at[owner, pl.ds(out_first_other, out_rows)]
        remote(part, part, core_send.at[k], core_recv.at[k], {"ep": other}).wait_recv()

    @pl.when(core == 0)
    def _():
        core_own().wait_send()

    @pl.when(core == 1)
    def _():
        kv_copy(z, 0, core_send.at[3], core_recv.at[3], {"ep": other}).wait_recv()

    for copy in own:
        copy.wait()

    @pl.when(is_self)
    def _():
        row_local().wait()


def fwd_copy_in(kv_copy, kv_all, z, n_z, core, s, send, recv, up_ep):
    kv_copy(
        lax.rem(z - 1 - s + n_z, n_z), core, send.at[s], recv.at[s], {"ep": up_ep}
    ).wait_recv()


def bwd_copy_in(kv_copy, z, n_z, core, s, send, recv, down_ep):
    kv_copy(lax.rem(z + 1 + s, n_z), core, send.at[s], recv.at[s], {"ep": down_ep}).wait_recv()


def split_three(value):
    high = value.astype(BF16)
    rest = value - high.astype(F32)
    mid = rest.astype(BF16)
    low = (rest - mid.astype(F32)).astype(BF16)
    return high.astype(F32), mid.astype(F32), low.astype(F32)


def attention_kernel(
    heads,
    query_ref,
    gain_ref,
    forget_ref,
    kv_ref,
    out_ref,
    query_t,
    run_max,
    run_sum,
    acc,
):
    span = query_ref.shape[0]
    me = lax.axis_index("ep")
    scale = HEAD_SIZE ** (-0.5)
    exp_scale = scale * LOG2E
    columns = heads * span
    for h in range(heads):
        normed = row_norm(query_ref[:, h * HEAD_SIZE : (h + 1) * HEAD_SIZE], gain_ref[...])
        rounded = normed.astype(BF16).astype(F32)
        query_t[:HEAD_SIZE, h * span : (h + 1) * span] = rounded.T.astype(BF16)
    row = lax.broadcasted_iota(jnp.int32, (HEAD_SIZE, columns), 0)
    head = lax.broadcasted_iota(jnp.int32, (HEAD_SIZE, columns), 1) // span
    query_t[HEAD_SIZE:, :] = jnp.where(row // 3 == head, 1.0, 0.0).astype(BF16)
    run_max[...] = jnp.full(run_max.shape, -1e30, F32)
    run_sum[...] = jnp.zeros(run_sum.shape, F32)
    acc[...] = jnp.zeros(acc.shape, F32)
    lane = lax.broadcasted_iota(jnp.int32, (8, HEAD_SIZE), 1)
    sub = lax.broadcasted_iota(jnp.int32, (8, HEAD_SIZE), 0)
    place = jnp.where(lane == sub, 1.0, 0.0).astype(BF16)
    width = 256

    def add_block(block, masked):
        first = pl.multiple_of(block * span, span)
        rows = []
        for h in range(heads):
            gates = forget_ref[h : h + 1, pl.ds(first, span)]
            rows.extend(split_three(gates * (-1.0 / scale)))
        rows.append(jnp.zeros((8 - len(rows), span), F32))
        stacked = jnp.concatenate(rows, axis=0).astype(BF16)
        bias = dot(stacked, place, (((0,), (0,)), ((), ()))).astype(BF16)
        keys = jnp.concatenate([kv_ref[block, :, :HEAD_SIZE], bias], axis=1)
        values = kv_ref[block, :, HEAD_SIZE:]
        for first_col in range(0, columns, width):
            cols = slice(first_col, first_col + width)
            scores = dot(keys, query_t[:, cols])
            if masked:
                key_at = lax.broadcasted_iota(jnp.int32, (span, width), 0)
                query_at = lax.broadcasted_iota(jnp.int32, (span, width), 1) + first_col % span
                scores = jnp.where(key_at <= query_at, scores, -1e30)
            old_max = run_max[:, cols]
            new_max = jnp.maximum(old_max, jnp.max(scores, axis=0, keepdims=True))
            shrink = jnp.exp2((old_max - new_max) * exp_scale)
            weights = jnp.exp2((scores - new_max) * exp_scale)
            run_max[:, cols] = new_max
            run_sum[:, cols] = shrink * run_sum[:, cols] + jnp.sum(weights, axis=0, keepdims=True)
            gathered = dot(values, weights.astype(BF16), (((0,), (0,)), ((), ())))
            acc[:, cols] = shrink * acc[:, cols] + gathered

    def body(block, carry):
        add_block(block, False)
        return carry

    lax.fori_loop(0, me, body, 0)
    add_block(me, True)
    for h in range(heads):
        cols = slice(h * span, (h + 1) * span)
        attended = (acc[:, cols] / run_sum[:, cols]).T
        out_ref[:, h * HEAD_SIZE : (h + 1) * HEAD_SIZE] = attended.astype(BF16)


def expert_kernel(rows_ref, gate_ref, up_ref, down_ref, out_ref, total):
    p = pl.program_id(0)
    parts, sources = out_ref.shape[0], out_ref.shape[1]
    width = out_ref.shape[3]
    rows = rows_ref[...]
    gate = dot(rows, gate_ref[0])
    up = dot(rows, up_ref[0])
    hidden = (gate / (1.0 + jnp.exp(-gate)) * up).astype(BF16)

    @pl.when(p == 0)
    def _():
        total[...] = jnp.zeros(total.shape, F32)

    for q in range(parts):
        cols = slice(q * width, (q + 1) * width)
        piece = dot(hidden, down_ref[0, :, cols]).astype(BF16).astype(F32)
        total[:, cols] += piece

    @pl.when(p == pl.num_programs(0) - 1)
    def _():
        for q in range(parts):
            for n in range(sources):
                out_ref[q, n] = total[
                    n * CAP : (n + 1) * CAP, q * width : (q + 1) * width
                ].astype(BF16)


def return_kernel(
    n_ep,
    n_tp,
    result_ref,
    attended_ref,
    back_ref,
    heads_ref,
    row_send,
    row_recv,
    head_send,
    head_recv,
    local,
):
    me, t = lax.axis_index("ep"), lax.axis_index("tp")
    offset = lax.rem(t + (n_tp - 1) * me, n_tp)
    here = n_ep // n_tp
    token_rows = attended_ref.shape[0] // n_tp
    self_slot = me // n_tp
    is_self = lax.rem(me, n_tp) == offset

    barrier = pltpu.get_barrier_semaphore()
    for e in range(n_ep):
        column = lax.rem(me + e, n_tp)

        @pl.when(jnp.logical_not(jnp.logical_and(me == e, column == t)))
        def _(e=e, column=column):
            pl.semaphore_signal(
                barrier, inc=1, device_id={"ep": e, "tp": column}, device_id_type=MESH
            )

    for k in range(1, n_tp):
        pl.semaphore_signal(
            barrier, inc=1, device_id={"tp": lax.rem(t + k, n_tp)}, device_id_type=MESH
        )
    pl.semaphore_wait(barrier, n_ep + n_tp - 1 - jnp.where(is_self, 1, 0))

    def remote(src, dst, send_sem, recv_sem, where):
        return pltpu.make_async_remote_copy(
            src_ref=src,
            dst_ref=dst,
            send_sem=send_sem,
            recv_sem=recv_sem,
            device_id=where,
            device_id_type=MESH,
        )

    def head_copy(k):
        q = lax.rem(t + k, n_tp)
        first = pl.multiple_of(q * token_rows, token_rows)
        return remote(
            attended_ref.at[pl.ds(first, token_rows)],
            heads_ref.at[t],
            head_send.at[k],
            head_recv.at[k],
            {"tp": q},
        )

    own_first = pl.multiple_of(t * token_rows, token_rows)
    own_heads = pltpu.make_async_copy(
        attended_ref.at[pl.ds(own_first, token_rows)], heads_ref.at[t], local.at[0]
    )
    own_row = pltpu.make_async_copy(result_ref.at[t, self_slot], back_ref.at[me], local.at[1])

    def row_copy(k, j):
        n = lax.rem(self_slot + k, here)
        q = lax.rem(t + j, n_tp)
        target = offset + n_tp * n
        away = jnp.logical_not(jnp.logical_and(target == me, q == t))
        return away, remote(
            result_ref.at[q, n],
            back_ref.at[me],
            row_send.at[k, j],
            row_recv.at[me],
            {"ep": target, "tp": q},
        )

    for k in range(1, n_tp):
        head_copy(k).start()
    own_heads.start()

    @pl.when(is_self)
    def _():
        own_row.start()

    for k in range(here):
        for j in range(n_tp):
            away, copy = row_copy(k, j)

            @pl.when(away)
            def _(copy=copy):
                copy.start()

    for k in range(here):
        for j in range(n_tp):
            away, copy = row_copy(k, j)

            @pl.when(away)
            def _(copy=copy):
                copy.wait_send()

    for e in range(n_ep):
        column = lax.rem(me + e, n_tp)
        arrival = remote(
            result_ref.at[0, 0],
            back_ref.at[e],
            row_send.at[0, 0],
            row_recv.at[e],
            {"ep": e, "tp": column},
        )

        @pl.when(jnp.logical_not(jnp.logical_and(me == e, column == t)))
        def _(arrival=arrival):
            arrival.wait_recv()

    for k in range(1, n_tp):
        source = lax.rem(t + n_tp - k, n_tp)
        head_copy(k).wait_send()
        remote(
            attended_ref.at[pl.ds(0, token_rows)],
            heads_ref.at[source],
            head_send.at[k],
            head_recv.at[k],
            {"tp": source},
        ).wait_recv()
    own_heads.wait()

    @pl.when(is_self)
    def _():
        own_row.wait()


def combine_kernel(back_ref, routes_ref, weight_ref, heads_ref, out_w_ref, mixer_ref, out_ref):
    slots = back_ref.shape[0]
    span = routes_ref.shape[1]
    expert_col = lax.broadcasted_iota(jnp.int32, (EXPERTS, 1), 0)
    routes = routes_ref[...]
    _, rank = member_and_rank(routes, expert_col)
    total = None
    for j in range(TOP):
        chosen = routes[j : j + 1, :]
        within = jnp.sum(jnp.where(chosen == expert_col, rank, 0.0), axis=0, keepdims=True)
        slot = chosen * CAP + within.astype(jnp.int32)
        at = lax.broadcasted_iota(jnp.int32, (slots, span), 0)
        pick = jnp.where(at == slot, 1.0, 0.0).astype(BF16)
        picked = dot(pick, back_ref[...], (((0,), (0,)), ((), ())))
        term = picked * weight_ref[:, j : j + 1]
        total = term if total is None else total + term
    out_ref[...] = total.astype(BF16)
    projected = None
    for k in range(heads_ref.shape[0]):
        piece = dot(heads_ref[k], out_w_ref[k])
        projected = piece if projected is None else projected + piece
    mixer_ref[...] = projected.astype(BF16)


def on_device(
    n_ep,
    n_tp,
    queries,
    key_rows,
    value_rows,
    query_gain,
    key_gain,
    log_forget,
    out_weight,
    expert_rows,
    expert_gain,
    routes,
    route_weight,
    gate_weight,
    up_weight,
    down_weight,
):
    span, model_width = expert_rows.shape
    here = n_ep // n_tp
    heads = queries.shape[1] // HEAD_SIZE
    width = model_width // n_tp
    n_z = n_ep // CORES
    reach = n_z // 2
    ff_part = gate_weight.shape[2]
    hbm = pl.BlockSpec(memory_space=pltpu.HBM)
    vmem = pl.BlockSpec(memory_space=pltpu.VMEM)
    shape = jax.ShapeDtypeStruct
    big = pltpu.CompilerParams(vmem_limit_bytes=56 * 1024 * 1024)

    send_rows, key_value = pl.pallas_call(
        functools.partial(prologue_kernel, n_tp),
        out_shape=(
            shape((here, CAP, model_width), BF16),
            shape((span, 2 * HEAD_SIZE), BF16),
        ),
        in_specs=[vmem] * 6,
        out_specs=(vmem, vmem),
        scratch_shapes=[pltpu.VMEM((span, model_width), BF16)],
        compiler_params=big,
        name="prologue",
    )(
        expert_rows,
        expert_gain.reshape(1, -1),
        routes,
        key_rows,
        value_rows,
        key_gain.reshape(1, -1),
    )

    dma = pltpu.SemaphoreType.DMA
    recv_rows, kv_all, gate_all, up_all, down_all, out_all = pl.pallas_call(
        functools.partial(spread_kernel, n_ep, n_tp),
        out_shape=(
            shape((here, CAP, model_width), BF16),
            shape((n_ep, span, 2 * HEAD_SIZE), BF16),
            shape((n_tp, model_width, ff_part), BF16),
            shape((n_tp, model_width, ff_part), BF16),
            shape((n_tp, ff_part, model_width), BF16),
            shape((n_tp, *out_weight.shape), BF16),
        ),
        in_specs=[hbm] * 6,
        out_specs=(hbm,) * 6,
        scratch_shapes=[
            dma((here,)),
            dma((here,)),
            dma((reach,)),
            dma((reach,)),
            dma((reach - 1,)),
            dma((reach - 1,)),
            dma((4 + 2 * reach,)),
            dma((4 + 2 * reach,)),
            dma((4, 2)),
            dma((4, 2)),
            dma((4, 2)),
            dma((4, 2)),
            dma((6,)),
        ],
        compiler_params=pltpu.CompilerParams(collective_id=0, has_side_effects=True),
        name="spread",
    )(
        send_rows,
        key_value,
        gate_weight.reshape(model_width, ff_part),
        up_weight.reshape(model_width, ff_part),
        down_weight.reshape(ff_part, model_width),
        out_weight,
    )

    results = pl.pallas_call(
        expert_kernel,
        grid=(n_tp,),
        out_shape=shape((n_tp, here, CAP, width), BF16),
        in_specs=[
            pl.BlockSpec((here * CAP, model_width), lambda p: (0, 0)),
            pl.BlockSpec((1, model_width, ff_part), lambda p: (p, 0, 0)),
            pl.BlockSpec((1, model_width, ff_part), lambda p: (p, 0, 0)),
            pl.BlockSpec((1, ff_part, model_width), lambda p: (p, 0, 0)),
        ],
        out_specs=pl.BlockSpec((n_tp, here, CAP, width), lambda p: (0, 0, 0, 0)),
        scratch_shapes=[pltpu.VMEM((here * CAP, model_width), F32)],
        compiler_params=pltpu.CompilerParams(
            dimension_semantics=("arbitrary",), vmem_limit_bytes=56 * 1024 * 1024
        ),
        name="experts",
    )(recv_rows.reshape(here * CAP, model_width), gate_all, up_all, down_all)

    columns = heads * span
    attended = pl.pallas_call(
        functools.partial(attention_kernel, heads),
        out_shape=shape((span, heads * HEAD_SIZE), BF16),
        in_specs=[vmem] * 4,
        out_specs=vmem,
        scratch_shapes=[
            pltpu.VMEM((2 * HEAD_SIZE, columns), BF16),
            pltpu.VMEM((1, columns), F32),
            pltpu.VMEM((1, columns), F32),
            pltpu.VMEM((HEAD_SIZE, columns), F32),
        ],
        compiler_params=big,
        name="attention",
    )(queries, query_gain.reshape(1, -1), log_forget, kv_all)

    back_rows, head_rows = pl.pallas_call(
        functools.partial(return_kernel, n_ep, n_tp),
        out_shape=(
            shape((n_ep, CAP, width), BF16),
            shape((n_tp, span // n_tp, heads * HEAD_SIZE), BF16),
        ),
        in_specs=[hbm] * 2,
        out_specs=(hbm, hbm),
        scratch_shapes=[
            dma((here, n_tp)),
            dma((n_ep,)),
            dma((n_tp,)),
            dma((n_tp,)),
            dma((2,)),
        ],
        compiler_params=pltpu.CompilerParams(collective_id=1, has_side_effects=True),
        name="give_back",
    )(results, attended)

    mixer_out, expert_out = pl.pallas_call(
        combine_kernel,
        out_shape=(
            shape((span // n_tp, model_width), BF16),
            shape((span, width), BF16),
        ),
        in_specs=[vmem] * 5,
        out_specs=(vmem, vmem),
        compiler_params=big,
        name="combine",
    )(back_rows.reshape(n_ep * CAP, width), routes, route_weight.T, head_rows, out_all)
    return (mixer_out, expert_out)


def solution(mesh):
    in_specs = (
        P(("grp", "ep"), "tp"),
        P(("grp", "ep"), "tp"),
        P(("grp", "ep"), "tp"),
        P(),
        P(),
        P("tp", "grp"),
        P("tp", None),
        P(("grp", "ep"), None),
        P(),
        P(None, ("grp", "ep")),
        P(None, ("grp", "ep")),
        P("ep", None, "tp"),
        P("ep", None, "tp"),
        P("ep", "tp", None),
    )
    out_specs = (P(("grp", "ep", "tp"), None), P(("grp", "ep"), "tp"))
    return jax.shard_map(
        functools.partial(on_device, mesh.shape["ep"], mesh.shape["tp"]),
        mesh=mesh,
        in_specs=in_specs,
        out_specs=out_specs,
        check_vma=False,
    )
```

```python
import functools

import jax
import jax.numpy as jnp
from jax import lax
from jax.experimental import pallas as pl
from jax.experimental.pallas import tpu as pltpu
from jax.sharding import PartitionSpec as P

HEAD_SIZE = 128
EXPERTS = 32
CAP = 48
TOP = 2
CORES = 2
LOG2E = 1.4426950408889634
MESH = pl.DeviceIdType.MESH
F32 = jnp.float32
BF16 = jnp.bfloat16


def dot(a, b, dims=(((1,), (0,)), ((), ()))):
    return lax.dot_general(a, b, dims, preferred_element_type=F32)


def row_norm(rows, gain):
    wide = rows.astype(F32)
    factor = lax.rsqrt(jnp.mean(wide * wide, axis=-1, keepdims=True) + 1e-06)
    return wide * factor * gain


def member_and_rank(routes, expert_col):
    tokens = routes.shape[1]
    count = expert_col.shape[0]
    named = jnp.logical_or(routes[0:1, :] == expert_col, routes[1:2, :] == expert_col)
    member = jnp.where(named, 1.0, 0.0).astype(F32)
    before = lax.broadcasted_iota(jnp.int32, (tokens, tokens), 0)
    after = lax.broadcasted_iota(jnp.int32, (tokens, tokens), 1)
    earlier = jnp.where(before < after, 1.0, 0.0).astype(BF16)
    del count
    return member, dot(member.astype(BF16), earlier)


def prologue_kernel(
    n_tp,
    rows_ref,
    gain_ref,
    routes_ref,
    key_ref,
    value_ref,
    key_gain_ref,
    send_ref,
    own_key_ref,
    own_value_ref,
    normed,
):
    span = rows_ref.shape[0]
    me, t = lax.axis_index("ep"), lax.axis_index("tp")
    offset = lax.rem(t + (n_tp - 1) * me, n_tp)
    own_key_ref[...] = row_norm(key_ref[...], key_gain_ref[...]).astype(BF16)
    own_value_ref[...] = value_ref[...].astype(F32).T.astype(BF16)
    step = 64
    for first in range(0, span, step):
        normed[first : first + step, :] = row_norm(
            rows_ref[first : first + step, :], gain_ref[...]
        ).astype(BF16)
    here = EXPERTS // n_tp
    expert_col = offset + n_tp * lax.broadcasted_iota(jnp.int32, (here, 1), 0)
    member, rank = member_and_rank(routes_ref[...], expert_col)
    place = jnp.where(member > 0.5, rank, -1.0)
    slot = lax.broadcasted_iota(jnp.int32, (CAP, span), 0).astype(F32)
    for m in range(here):
        pick = jnp.where(place[m : m + 1, :] == slot, 1.0, 0.0).astype(BF16)
        send_ref[m] = dot(pick, normed[...]).astype(BF16)


def split_three(value):
    high = value.astype(BF16)
    rest = value - high.astype(F32)
    mid = rest.astype(BF16)
    low = (rest - mid.astype(F32)).astype(BF16)
    return high.astype(F32), mid.astype(F32), low.astype(F32)


def prepare_attention(
    heads, blocks, query_ref, gain_ref, forget_ref, query_t, bias, run_max, run_sum, acc
):
    span = query_ref.shape[0]
    columns = heads * span
    for h in range(heads):
        normed = row_norm(query_ref[:, h * HEAD_SIZE : (h + 1) * HEAD_SIZE], gain_ref[...])
        rounded = normed.astype(BF16).astype(F32)
        query_t[:HEAD_SIZE, h * span : (h + 1) * span] = rounded.T.astype(BF16)
    row = lax.broadcasted_iota(jnp.int32, (HEAD_SIZE, columns), 0)
    head = lax.broadcasted_iota(jnp.int32, (HEAD_SIZE, columns), 1) // span
    query_t[HEAD_SIZE:, :] = jnp.where(row // 3 == head, 1.0, 0.0).astype(BF16)
    run_max[...] = jnp.full(run_max.shape, -1e30, F32)
    run_sum[...] = jnp.zeros(run_sum.shape, F32)
    acc[...] = jnp.zeros(acc.shape, F32)
    lane = lax.broadcasted_iota(jnp.int32, (8, HEAD_SIZE), 1)
    sub = lax.broadcasted_iota(jnp.int32, (8, HEAD_SIZE), 0)
    place = jnp.where(lane == sub, 1.0, 0.0).astype(BF16)

    def one(block, carry):
        first = pl.multiple_of(block * span, span)
        rows = []
        for h in range(heads):
            gates = forget_ref[h : h + 1, pl.ds(first, span)]
            rows.extend(split_three(gates * (-(HEAD_SIZE**0.5))))
        rows.append(jnp.zeros((8 - len(rows), span), F32))
        stacked = jnp.concatenate(rows, axis=0).astype(BF16)
        bias[block] = dot(stacked, place, (((0,), (0,)), ((), ()))).astype(BF16)
        return carry

    lax.fori_loop(0, blocks, one, 0)


def attend_block(block, masked, keys_all, values_all, query_t, bias, run_max, run_sum, acc):
    span = keys_all.shape[1]
    columns = query_t.shape[1]
    exp_scale = HEAD_SIZE ** (-0.5) * LOG2E
    width = 256
    keys = jnp.concatenate([keys_all[block], bias[block]], axis=1)
    values = values_all[block]
    for first_col in range(0, columns, width):
        cols = slice(first_col, first_col + width)
        scores = dot(keys, query_t[:, cols])
        if masked:
            key_at = lax.broadcasted_iota(jnp.int32, (span, width), 0)
            query_at = lax.broadcasted_iota(jnp.int32, (span, width), 1) + first_col % span
            scores = jnp.where(key_at <= query_at, scores, -1e30)
        old_max = run_max[:, cols]
        new_max = jnp.maximum(old_max, jnp.max(scores, axis=0, keepdims=True))
        shrink = jnp.exp2((old_max - new_max) * exp_scale)
        weights = jnp.exp2((scores - new_max) * exp_scale)
        run_max[:, cols] = new_max
        run_sum[:, cols] = shrink * run_sum[:, cols] + jnp.sum(weights, axis=0, keepdims=True)
        acc[:, cols] = shrink * acc[:, cols] + dot(values, weights.astype(BF16))


def finish_attention(heads, out_ref, run_sum, acc):
    span = out_ref.shape[0]
    for h in range(heads):
        cols = slice(h * span, (h + 1) * span)
        attended = (acc[:, cols] / run_sum[:, cols]).T
        out_ref[:, h * HEAD_SIZE : (h + 1) * HEAD_SIZE] = attended.astype(BF16)


def remote(src, dst, send_sem, recv_sem, where):
    return pltpu.make_async_remote_copy(
        src_ref=src,
        dst_ref=dst,
        send_sem=send_sem,
        recv_sem=recv_sem,
        device_id=where,
        device_id_type=MESH,
    )


def spread_kernel(
    n_ep,
    n_tp,
    heads,
    send_ref,
    key_ref,
    value_ref,
    query_ref,
    query_gain_ref,
    forget_ref,
    gate_ref,
    up_ref,
    down_ref,
    recv_ref,
    gate_all,
    up_all,
    down_all,
    attended_ref,
    keys_all,
    values_all,
    query_t,
    bias,
    run_max,
    run_sum,
    acc,
    gate_own,
    up_own,
    down_own,
    row_own,
    row_send,
    row_recv,
    fwd_send,
    fwd_recv,
    bwd_send,
    bwd_recv,
    core_send,
    core_recv,
    side_send,
    side_recv,
    half_send,
    half_recv,
    local,
):
    me, t = lax.axis_index("ep"), lax.axis_index("tp")
    n_z = n_ep // CORES
    z, core = me // CORES, lax.rem(me, CORES)
    offset = lax.rem(t + (n_tp - 1) * me, n_tp)
    here = n_ep // n_tp
    right, left = lax.rem(t + 1, n_tp), lax.rem(t + n_tp - 1, n_tp)
    up_ep = CORES * lax.rem(z + 1, n_z) + core
    down_ep = CORES * lax.rem(z + n_z - 1, n_z) + core
    other = CORES * z + (1 - core)
    reach = n_z // 2
    self_slot = me // n_tp
    is_self = lax.rem(me, n_tp) == offset

    barrier = pltpu.get_barrier_semaphore()
    for where in (
        {"ep": up_ep},
        {"ep": down_ep},
        {"ep": other},
        {"tp": right},
        {"tp": left},
    ):
        pl.semaphore_signal(barrier, inc=1, device_id=where, device_id_type=MESH)
    for m in range(here):
        mate = offset + n_tp * m

        @pl.when(mate != me)
        def _(mate=mate):
            pl.semaphore_signal(barrier, inc=1, device_id={"ep": mate}, device_id_type=MESH)

    pl.semaphore_wait(barrier, 5 + here - jnp.where(is_self, 1, 0))

    weights = (
        (gate_ref, gate_all, gate_own),
        (up_ref, up_all, up_own),
        (down_ref, down_all, down_own),
    )

    def side_copy(a, way):
        where = {"tp": (right, left)[way]}
        return remote(
            weights[a][0], weights[a][1].at[t], side_send.at[a, way], side_recv.at[a, way], where
        )

    def half_copy(a, way):
        where = {"tp": (right, left)[way]}
        owner = (left, right)[way]
        full = weights[a][1]
        half = full.shape[1] // 2
        part = full.at[owner, pl.ds(way * half, half)]
        return remote(part, part, half_send.at[a, way], half_recv.at[a, way], where)

    def hand_on(a):
        for way in range(2):
            side_copy(a, way).wait_recv()
            half_copy(a, way).start()

    own = [
        (
            pltpu.make_async_copy(src, held, local.at[a]),
            pltpu.make_async_copy(held, full.at[t], local.at[a]),
        )
        for a, (src, full, held) in enumerate(weights)
    ]
    own_row = (
        pltpu.make_async_copy(send_ref.at[self_slot], row_own, local.at[3]),
        pltpu.make_async_copy(row_own, recv_ref.at[self_slot], local.at[3]),
    )

    def block_copy(part, source_z, source_core, send_sem, recv_sem, where, mine=False):
        block = (keys_all, values_all)[part].at[CORES * source_z + source_core]
        return remote((key_ref, value_ref)[part] if mine else block, block, send_sem, recv_sem, where)

    def fwd_copy(s, part):
        source = lax.rem(z - s + n_z, n_z)
        sems = fwd_send.at[s, part], fwd_recv.at[s, part]
        return block_copy(part, source, core, *sems, {"ep": up_ep}, s == 0)

    def fwd_arrival(s, part):
        source = lax.rem(z - 1 - s + n_z, n_z)
        sems = fwd_send.at[s, part], fwd_recv.at[s, part]
        return block_copy(part, source, core, *sems, {"ep": up_ep})

    def bwd_copy(s, part):
        sems = bwd_send.at[s, part], bwd_recv.at[s, part]
        return block_copy(part, lax.rem(z + s, n_z), core, *sems, {"ep": down_ep}, s == 0)

    def bwd_arrival(s, part):
        sems = bwd_send.at[s, part], bwd_recv.at[s, part]
        return block_copy(part, lax.rem(z + 1 + s, n_z), core, *sems, {"ep": down_ep})

    def core_copy(k, part, source_z, source_core, mine=False):
        sems = core_send.at[k, part], core_recv.at[k, part]
        return block_copy(part, source_z, source_core, *sems, {"ep": other}, mine)

    def core_fwd(s, part, source_core):
        return core_copy(1 + s, part, lax.rem(z - 1 - s + n_z, n_z), source_core)

    def core_bwd(s, part, source_core):
        return core_copy(1 + reach + s, part, lax.rem(z + 1 + s, n_z), source_core)

    def fwd_sends(s):
        return jnp.logical_and(z - s >= 0, z + 1 <= n_z - 1)

    def fwd_gets(s):
        return z - 1 - s >= 0

    def bwd_sends(s):
        return lax.rem(z + s, n_z) <= reach - 2

    def bwd_gets(s):
        return lax.rem(z + 1 + s, n_z) <= reach - 2

    def bwd_needed(s):
        return jnp.logical_and(bwd_gets(s), lax.rem(z + 1 + s, n_z) < z)

    def row_copy(k):
        m = lax.rem(self_slot + k, here)
        mate = offset + n_tp * m
        return mate, remote(
            send_ref.at[m],
            recv_ref.at[self_slot],
            row_send.at[m],
            row_recv.at[self_slot],
            {"ep": mate},
        )

    for a in range(3):
        for way in range(2):
            side_copy(a, way).start()

    for part in range(2):

        @pl.when(fwd_sends(0))
        def _(part=part):
            fwd_copy(0, part).start()

        @pl.when(bwd_sends(0))
        def _(part=part):
            bwd_copy(0, part).start()

        @pl.when(core == 0)
        def _(part=part):
            core_copy(0, part, z, 0, True).start()

    for copies in own:
        copies[0].start()

    @pl.when(is_self)
    def _():
        own_row[0].start()

    keys_all[me] = key_ref[...]
    values_all[me] = value_ref[...]
    prepare_attention(
        heads, me + 1, query_ref, query_gain_ref, forget_ref, query_t, bias, run_max, run_sum, acc
    )
    for copies in own:
        copies[0].wait()
        copies[1].start()

    @pl.when(is_self)
    def _():
        own_row[0].wait()
        own_row[1].start()

    for s in range(reach):
        for part in range(2):

            @pl.when(fwd_gets(s))
            def _(s=s, part=part):
                fwd_arrival(s, part).wait_recv()

            if s + 1 < reach:

                @pl.when(fwd_sends(s + 1))
                def _(s=s, part=part):
                    fwd_copy(s + 1, part).start()

            @pl.when(fwd_gets(s))
            def _(s=s, part=part):
                core_fwd(s, part, core).start()

            if s < reach - 1:

                @pl.when(bwd_gets(s))
                def _(s=s, part=part):
                    bwd_arrival(s, part).wait_recv()

                if s + 1 < reach - 1:

                    @pl.when(bwd_sends(s + 1))
                    def _(s=s, part=part):
                        bwd_copy(s + 1, part).start()

                @pl.when(bwd_needed(s))
                def _(s=s, part=part):
                    core_bwd(s, part, core).start()

        if s == reach // 2:
            hand_on(0)

    for k in range(here):
        mate, copy = row_copy(k)

        @pl.when(mate != me)
        def _(copy=copy):
            copy.start()

    hand_on(1)

    for part in range(2):

        @pl.when(core == 1)
        def _(part=part):
            core_copy(0, part, z, 0).wait_recv()

        for s in range(reach):

            @pl.when(fwd_gets(s))
            def _(s=s, part=part):
                core_fwd(s, part, 1 - core).wait_recv()

            if s < reach - 1:

                @pl.when(bwd_needed(s))
                def _(s=s, part=part):
                    core_bwd(s, part, 1 - core).wait_recv()

    state = (keys_all, values_all, query_t, bias, run_max, run_sum, acc)

    def body(block, carry):
        attend_block(block, False, *state)
        return carry

    middle = me // 2
    lax.fori_loop(0, middle, body, 0)
    hand_on(2)
    lax.fori_loop(middle, me, body, 0)
    attend_block(me, True, *state)
    finish_attention(heads, attended_ref, run_sum, acc)

    for a in range(3):
        for way in range(2):
            side_copy(a, way).wait_send()
            half_copy(a, way).wait_recv()
            half_copy(a, way).wait_send()
    for k in range(here):
        mate, copy = row_copy(k)

        @pl.when(mate != me)
        def _(copy=copy):
            copy.wait_send()

        source = offset + n_tp * k
        arrival = remote(
            send_ref.at[k], recv_ref.at[k], row_send.at[k], row_recv.at[k], {"ep": source}
        )

        @pl.when(source != me)
        def _(arrival=arrival):
            arrival.wait_recv()

    for part in range(2):

        @pl.when(core == 0)
        def _(part=part):
            core_copy(0, part, z, 0, True).wait_send()

        for s in range(reach):

            @pl.when(fwd_sends(s))
            def _(s=s, part=part):
                fwd_copy(s, part).wait_send()

            @pl.when(fwd_gets(s))
            def _(s=s, part=part):
                core_fwd(s, part, core).wait_send()

            if s < reach - 1:

                @pl.when(bwd_sends(s))
                def _(s=s, part=part):
                    bwd_copy(s, part).wait_send()

                @pl.when(bwd_needed(s))
                def _(s=s, part=part):
                    core_bwd(s, part, core).wait_send()

    for copies in own:
        copies[1].wait()

    @pl.when(is_self)
    def _():
        own_row[1].wait()


def expert_kernel(rows_ref, gate_ref, up_ref, down_ref, out_ref, total):
    p = pl.program_id(0)
    parts, sources = out_ref.shape[0], out_ref.shape[1]
    width = out_ref.shape[3]
    rows = rows_ref[...]
    gate = dot(rows, gate_ref[0])
    up = dot(rows, up_ref[0])
    hidden = (gate / (1.0 + jnp.exp(-gate)) * up).astype(BF16)

    @pl.when(p == 0)
    def _():
        total[...] = jnp.zeros(total.shape, F32)

    for q in range(parts):
        cols = slice(q * width, (q + 1) * width)
        piece = dot(hidden, down_ref[0, :, cols]).astype(BF16).astype(F32)
        total[:, cols] += piece

    @pl.when(p == pl.num_programs(0) - 1)
    def _():
        for q in range(parts):
            for n in range(sources):
                out_ref[q, n] = total[
                    n * CAP : (n + 1) * CAP, q * width : (q + 1) * width
                ].astype(BF16)


def return_kernel(
    n_ep,
    n_tp,
    result_ref,
    attended_ref,
    out_ref,
    back_ref,
    heads_ref,
    out_all,
    out_own,
    row_send,
    row_recv,
    head_send,
    head_recv,
    side_send,
    side_recv,
    core_send,
    core_recv,
    local,
):
    me, t = lax.axis_index("ep"), lax.axis_index("tp")
    offset = lax.rem(t + (n_tp - 1) * me, n_tp)
    here = n_ep // n_tp
    token_rows = attended_ref.shape[0] // n_tp
    self_slot = me // n_tp
    is_self = lax.rem(me, n_tp) == offset

    barrier = pltpu.get_barrier_semaphore()
    for e in range(n_ep):
        column = lax.rem(me + e, n_tp)

        @pl.when(jnp.logical_not(jnp.logical_and(me == e, column == t)))
        def _(e=e, column=column):
            pl.semaphore_signal(
                barrier, inc=1, device_id={"ep": e, "tp": column}, device_id_type=MESH
            )

    for k in range(1, n_tp):
        pl.semaphore_signal(
            barrier, inc=1, device_id={"tp": lax.rem(t + k, n_tp)}, device_id_type=MESH
        )
    core = lax.rem(me, CORES)
    other = me + 1 - 2 * core
    right, left = lax.rem(t + 1, n_tp), lax.rem(t + n_tp - 1, n_tp)
    across = lax.rem(t + 2, n_tp)
    pl.semaphore_signal(barrier, inc=1, device_id={"ep": other}, device_id_type=MESH)
    pl.semaphore_wait(barrier, n_ep + n_tp - jnp.where(is_self, 1, 0))

    out_rows = out_ref.shape[0] // CORES
    out_first = core * out_rows
    quarter = out_rows // 2

    def side_copy(way):
        mine = pl.ds(out_first, out_rows)
        where = {"tp": (right, left)[way]}
        return remote(
            out_ref.at[mine], out_all.at[t, mine], side_send.at[0, way], side_recv.at[0, way], where
        )

    def half_copy(way):
        where = {"tp": (right, left)[way]}
        owner = (left, right)[way]
        part = out_all.at[owner, pl.ds(out_first + way * quarter, quarter)]
        return remote(part, part, side_send.at[1, way], side_recv.at[1, way], where)

    def core_copy(k, first):
        part = out_all.at[(left, right, across)[k], pl.ds(first, out_rows)]
        return remote(part, part, core_send.at[k], core_recv.at[k], {"ep": other})

    own_out = (
        pltpu.make_async_copy(out_ref, out_own, local.at[2]),
        pltpu.make_async_copy(out_own, out_all.at[t], local.at[2]),
    )

    def head_copy(k):
        q = lax.rem(t + k, n_tp)
        first = pl.multiple_of(q * token_rows, token_rows)
        return remote(
            attended_ref.at[pl.ds(first, token_rows)],
            heads_ref.at[t],
            head_send.at[k],
            head_recv.at[k],
            {"tp": q},
        )

    own_first = pl.multiple_of(t * token_rows, token_rows)
    own_heads = pltpu.make_async_copy(
        attended_ref.at[pl.ds(own_first, token_rows)], heads_ref.at[t], local.at[0]
    )
    own_row = pltpu.make_async_copy(result_ref.at[t, self_slot], back_ref.at[me], local.at[1])

    def row_copy(k, j):
        n = lax.rem(self_slot + k, here)
        q = lax.rem(t + j, n_tp)
        target = offset + n_tp * n
        away = jnp.logical_not(jnp.logical_and(target == me, q == t))
        return away, remote(
            result_ref.at[q, n],
            back_ref.at[me],
            row_send.at[k, j],
            row_recv.at[me],
            {"ep": target, "tp": q},
        )

    for k in range(1, n_tp):
        head_copy(k).start()
    own_heads.start()

    @pl.when(is_self)
    def _():
        own_row.start()

    for k in range(here):
        for j in range(n_tp):
            away, copy = row_copy(k, j)

            @pl.when(away)
            def _(copy=copy):
                copy.start()

    for way in range(2):
        side_copy(way).start()
    own_out[0].start()
    own_out[0].wait()
    own_out[1].start()
    for way in range(2):
        side_copy(way).wait_recv()
        half_copy(way).start()
        core_copy(way, out_first).start()
    for way in range(2):
        half_copy(way).wait_recv()
    core_copy(2, out_first).start()
    for way in range(2):
        side_copy(way).wait_send()
        half_copy(way).wait_send()
    for k in range(3):
        core_copy(k, out_first).wait_send()
        core_copy(k, (1 - core) * out_rows).wait_recv()
    own_out[1].wait()

    for k in range(here):
        for j in range(n_tp):
            away, copy = row_copy(k, j)

            @pl.when(away)
            def _(copy=copy):
                copy.wait_send()

    for e in range(n_ep):
        column = lax.rem(me + e, n_tp)
        arrival = remote(
            result_ref.at[0, 0],
            back_ref.at[e],
            row_send.at[0, 0],
            row_recv.at[e],
            {"ep": e, "tp": column},
        )

        @pl.when(jnp.logical_not(jnp.logical_and(me == e, column == t)))
        def _(arrival=arrival):
            arrival.wait_recv()

    for k in range(1, n_tp):
        source = lax.rem(t + n_tp - k, n_tp)
        head_copy(k).wait_send()
        remote(
            attended_ref.at[pl.ds(0, token_rows)],
            heads_ref.at[source],
            head_send.at[k],
            head_recv.at[k],
            {"tp": source},
        ).wait_recv()
    own_heads.wait()

    @pl.when(is_self)
    def _():
        own_row.wait()


def combine_kernel(back_ref, routes_ref, weight_ref, heads_ref, out_w_ref, mixer_ref, out_ref):
    slots = back_ref.shape[0]
    span = routes_ref.shape[1]
    expert_col = lax.broadcasted_iota(jnp.int32, (EXPERTS, 1), 0)
    routes = routes_ref[...]
    _, rank = member_and_rank(routes, expert_col)
    total = None
    for j in range(TOP):
        chosen = routes[j : j + 1, :]
        within = jnp.sum(jnp.where(chosen == expert_col, rank, 0.0), axis=0, keepdims=True)
        slot = chosen * CAP + within.astype(jnp.int32)
        at = lax.broadcasted_iota(jnp.int32, (slots, span), 0)
        pick = jnp.where(at == slot, 1.0, 0.0).astype(BF16)
        picked = dot(pick, back_ref[...], (((0,), (0,)), ((), ())))
        term = picked * weight_ref[:, j : j + 1]
        total = term if total is None else total + term
    out_ref[...] = total.astype(BF16)
    projected = None
    for k in range(heads_ref.shape[0]):
        piece = dot(heads_ref[k], out_w_ref[k])
        projected = piece if projected is None else projected + piece
    mixer_ref[...] = projected.astype(BF16)


def on_device(
    n_ep,
    n_tp,
    queries,
    key_rows,
    value_rows,
    query_gain,
    key_gain,
    log_forget,
    out_weight,
    expert_rows,
    expert_gain,
    routes,
    route_weight,
    gate_weight,
    up_weight,
    down_weight,
):
    span, model_width = expert_rows.shape
    here = n_ep // n_tp
    heads = queries.shape[1] // HEAD_SIZE
    width = model_width // n_tp
    n_z = n_ep // CORES
    reach = n_z // 2
    ff_part = gate_weight.shape[2]
    hbm = pl.BlockSpec(memory_space=pltpu.HBM)
    vmem = pl.BlockSpec(memory_space=pltpu.VMEM)
    shape = jax.ShapeDtypeStruct
    big = pltpu.CompilerParams(vmem_limit_bytes=56 * 1024 * 1024)

    send_rows, own_keys, own_values = pl.pallas_call(
        functools.partial(prologue_kernel, n_tp),
        out_shape=(
            shape((here, CAP, model_width), BF16),
            shape((span, HEAD_SIZE), BF16),
            shape((HEAD_SIZE, span), BF16),
        ),
        in_specs=[vmem] * 6,
        out_specs=(vmem,) * 3,
        scratch_shapes=[pltpu.VMEM((span, model_width), BF16)],
        compiler_params=big,
        name="prologue",
    )(
        expert_rows,
        expert_gain.reshape(1, -1),
        routes,
        key_rows,
        value_rows,
        key_gain.reshape(1, -1),
    )

    dma = pltpu.SemaphoreType.DMA
    columns = heads * span
    recv_rows, gate_all, up_all, down_all, attended = pl.pallas_call(
        functools.partial(spread_kernel, n_ep, n_tp, heads),
        out_shape=(
            shape((here, CAP, model_width), BF16),
            shape((n_tp, model_width, ff_part), BF16),
            shape((n_tp, model_width, ff_part), BF16),
            shape((n_tp, ff_part, model_width), BF16),
            shape((span, columns // span * HEAD_SIZE), BF16),
        ),
        in_specs=[hbm] + [vmem] * 5 + [hbm] * 3,
        out_specs=(hbm,) * 4 + (vmem,),
        scratch_shapes=[
            pltpu.VMEM((n_ep, span, HEAD_SIZE), BF16),
            pltpu.VMEM((n_ep, HEAD_SIZE, span), BF16),
            pltpu.VMEM((2 * HEAD_SIZE, columns), BF16),
            pltpu.VMEM((n_ep, span, HEAD_SIZE), BF16),
            pltpu.VMEM((1, columns), F32),
            pltpu.VMEM((1, columns), F32),
            pltpu.VMEM((HEAD_SIZE, columns), F32),
            pltpu.VMEM((model_width, ff_part), BF16),
            pltpu.VMEM((model_width, ff_part), BF16),
            pltpu.VMEM((ff_part, model_width), BF16),
            pltpu.VMEM((CAP, model_width), BF16),
            dma((here,)),
            dma((here,)),
            dma((reach, 2)),
            dma((reach, 2)),
            dma((reach - 1, 2)),
            dma((reach - 1, 2)),
            dma((2 * reach, 2)),
            dma((2 * reach, 2)),
            dma((3, 2)),
            dma((3, 2)),
            dma((3, 2)),
            dma((3, 2)),
            dma((4,)),
        ],
        compiler_params=pltpu.CompilerParams(
            collective_id=0, has_side_effects=True, vmem_limit_bytes=56 * 1024 * 1024
        ),
        name="spread",
    )(
        send_rows,
        own_keys,
        own_values,
        queries,
        query_gain.reshape(1, -1),
        log_forget,
        gate_weight.reshape(model_width, ff_part),
        up_weight.reshape(model_width, ff_part),
        down_weight.reshape(ff_part, model_width),
    )

    results = pl.pallas_call(
        expert_kernel,
        grid=(n_tp,),
        out_shape=shape((n_tp, here, CAP, width), BF16),
        in_specs=[
            pl.BlockSpec((here * CAP, model_width), lambda p: (0, 0)),
            pl.BlockSpec((1, model_width, ff_part), lambda p: (p, 0, 0)),
            pl.BlockSpec((1, model_width, ff_part), lambda p: (p, 0, 0)),
            pl.BlockSpec((1, ff_part, model_width), lambda p: (p, 0, 0)),
        ],
        out_specs=pl.BlockSpec((n_tp, here, CAP, width), lambda p: (0, 0, 0, 0)),
        scratch_shapes=[pltpu.VMEM((here * CAP, model_width), F32)],
        compiler_params=pltpu.CompilerParams(
            dimension_semantics=("arbitrary",), vmem_limit_bytes=56 * 1024 * 1024
        ),
        name="experts",
    )(recv_rows.reshape(here * CAP, model_width), gate_all, up_all, down_all)

    back_rows, head_rows, out_all = pl.pallas_call(
        functools.partial(return_kernel, n_ep, n_tp),
        out_shape=(
            shape((n_ep, CAP, width), BF16),
            shape((n_tp, span // n_tp, heads * HEAD_SIZE), BF16),
            shape((n_tp, *out_weight.shape), BF16),
        ),
        in_specs=[hbm] * 3,
        out_specs=(hbm,) * 3,
        scratch_shapes=[
            pltpu.VMEM(out_weight.shape, BF16),
            dma((here, n_tp)),
            dma((n_ep,)),
            dma((n_tp,)),
            dma((n_tp,)),
            dma((2, 2)),
            dma((2, 2)),
            dma((3,)),
            dma((3,)),
            dma((3,)),
        ],
        compiler_params=pltpu.CompilerParams(collective_id=1, has_side_effects=True),
        name="give_back",
    )(results, attended, out_weight)

    mixer_out, expert_out = pl.pallas_call(
        combine_kernel,
        out_shape=(
            shape((span // n_tp, model_width), BF16),
            shape((span, width), BF16),
        ),
        in_specs=[vmem] * 5,
        out_specs=(vmem, vmem),
        compiler_params=big,
        name="combine",
    )(back_rows.reshape(n_ep * CAP, width), routes, route_weight.T, head_rows, out_all)
    return (mixer_out, expert_out)


def solution(mesh):
    in_specs = (
        P(("grp", "ep"), "tp"),
        P(("grp", "ep"), "tp"),
        P(("grp", "ep"), "tp"),
        P(),
        P(),
        P("tp", "grp"),
        P("tp", None),
        P(("grp", "ep"), None),
        P(),
        P(None, ("grp", "ep")),
        P(None, ("grp", "ep")),
        P("ep", None, "tp"),
        P("ep", None, "tp"),
        P("ep", "tp", None),
    )
    out_specs = (P(("grp", "ep", "tp"), None), P(("grp", "ep"), "tp"))
    return jax.shard_map(
        functools.partial(on_device, mesh.shape["ep"], mesh.shape["tp"]),
        mesh=mesh,
        in_specs=in_specs,
        out_specs=out_specs,
        check_vma=False,
    )
```

```python
import functools

import jax
import jax.numpy as jnp
from jax import lax
from jax.experimental import pallas as pl
from jax.experimental.pallas import tpu as pltpu
from jax.sharding import PartitionSpec as P

HEAD_SIZE = 128
EXPERTS = 32
CAP = 48
TOP = 2
CORES = 2
LOG2E = 1.4426950408889634
MESH = pl.DeviceIdType.MESH
F32 = jnp.float32
BF16 = jnp.bfloat16


def dot(a, b, dims=(((1,), (0,)), ((), ()))):
    return lax.dot_general(a, b, dims, preferred_element_type=F32)


def row_norm(rows, gain):
    wide = rows.astype(F32)
    factor = lax.rsqrt(jnp.mean(wide * wide, axis=-1, keepdims=True) + 1e-06)
    return wide * factor * gain


def member_and_rank(routes, expert_col):
    tokens = routes.shape[1]
    count = expert_col.shape[0]
    named = jnp.logical_or(routes[0:1, :] == expert_col, routes[1:2, :] == expert_col)
    member = jnp.where(named, 1.0, 0.0).astype(F32)
    before = lax.broadcasted_iota(jnp.int32, (tokens, tokens), 0)
    after = lax.broadcasted_iota(jnp.int32, (tokens, tokens), 1)
    earlier = jnp.where(before < after, 1.0, 0.0).astype(BF16)
    del count
    return member, dot(member.astype(BF16), earlier)


def prologue_kernel(
    n_tp,
    rows_ref,
    gain_ref,
    routes_ref,
    key_ref,
    value_ref,
    key_gain_ref,
    send_ref,
    own_key_ref,
    own_value_ref,
    normed,
):
    span = rows_ref.shape[0]
    me, t = lax.axis_index("ep"), lax.axis_index("tp")
    offset = lax.rem(t + (n_tp - 1) * me, n_tp)
    own_key_ref[...] = row_norm(key_ref[...], key_gain_ref[...]).astype(BF16)
    own_value_ref[...] = value_ref[...].astype(F32).T.astype(BF16)
    step = 64
    for first in range(0, span, step):
        normed[first : first + step, :] = row_norm(
            rows_ref[first : first + step, :], gain_ref[...]
        ).astype(BF16)
    here = EXPERTS // n_tp
    expert_col = offset + n_tp * lax.broadcasted_iota(jnp.int32, (here, 1), 0)
    member, rank = member_and_rank(routes_ref[...], expert_col)
    place = jnp.where(member > 0.5, rank, -1.0)
    slot = lax.broadcasted_iota(jnp.int32, (CAP, span), 0).astype(F32)
    for m in range(here):
        pick = jnp.where(place[m : m + 1, :] == slot, 1.0, 0.0).astype(BF16)
        send_ref[m] = dot(pick, normed[...]).astype(BF16)


def split_three(value):
    high = value.astype(BF16)
    rest = value - high.astype(F32)
    mid = rest.astype(BF16)
    low = (rest - mid.astype(F32)).astype(BF16)
    return high.astype(F32), mid.astype(F32), low.astype(F32)


def prepare_attention(
    heads, blocks, query_ref, gain_ref, forget_ref, query_t, bias, run_max, run_sum, acc
):
    span = query_ref.shape[0]
    columns = heads * span
    for h in range(heads):
        normed = row_norm(query_ref[:, h * HEAD_SIZE : (h + 1) * HEAD_SIZE], gain_ref[...])
        rounded = normed.astype(BF16).astype(F32)
        query_t[:HEAD_SIZE, h * span : (h + 1) * span] = rounded.T.astype(BF16)
    row = lax.broadcasted_iota(jnp.int32, (HEAD_SIZE, columns), 0)
    head = lax.broadcasted_iota(jnp.int32, (HEAD_SIZE, columns), 1) // span
    query_t[HEAD_SIZE:, :] = jnp.where(row // 3 == head, 1.0, 0.0).astype(BF16)
    run_max[...] = jnp.full(run_max.shape, -1e30, F32)
    run_sum[...] = jnp.zeros(run_sum.shape, F32)
    acc[...] = jnp.zeros(acc.shape, F32)
    lane = lax.broadcasted_iota(jnp.int32, (8, HEAD_SIZE), 1)
    sub = lax.broadcasted_iota(jnp.int32, (8, HEAD_SIZE), 0)
    place = jnp.where(lane == sub, 1.0, 0.0).astype(BF16)

    def one(block, carry):
        first = pl.multiple_of(block * span, span)
        rows = []
        for h in range(heads):
            gates = forget_ref[h : h + 1, pl.ds(first, span)]
            rows.extend(split_three(gates * (-(HEAD_SIZE**0.5))))
        rows.append(jnp.zeros((8 - len(rows), span), F32))
        stacked = jnp.concatenate(rows, axis=0).astype(BF16)
        bias[block] = dot(stacked, place, (((0,), (0,)), ((), ()))).astype(BF16)
        return carry

    lax.fori_loop(0, blocks, one, 0)


def attend_block(block, masked, keys_all, values_all, query_t, bias, run_max, run_sum, acc):
    span = keys_all.shape[1]
    columns = query_t.shape[1]
    exp_scale = HEAD_SIZE ** (-0.5) * LOG2E
    width = 256
    keys = jnp.concatenate([keys_all[block], bias[block]], axis=1)
    values = values_all[block]
    for first_col in range(0, columns, width):
        cols = slice(first_col, first_col + width)
        scores = dot(keys, query_t[:, cols])
        if masked:
            key_at = lax.broadcasted_iota(jnp.int32, (span, width), 0)
            query_at = lax.broadcasted_iota(jnp.int32, (span, width), 1) + first_col % span
            scores = jnp.where(key_at <= query_at, scores, -1e30)
        old_max = run_max[:, cols]
        new_max = jnp.maximum(old_max, jnp.max(scores, axis=0, keepdims=True))
        shrink = jnp.exp2((old_max - new_max) * exp_scale)
        weights = jnp.exp2((scores - new_max) * exp_scale)
        run_max[:, cols] = new_max
        run_sum[:, cols] = shrink * run_sum[:, cols] + jnp.sum(weights, axis=0, keepdims=True)
        acc[:, cols] = shrink * acc[:, cols] + dot(values, weights.astype(BF16))


def finish_attention(heads, out_ref, run_sum, acc):
    span = out_ref.shape[0]
    for h in range(heads):
        cols = slice(h * span, (h + 1) * span)
        attended = (acc[:, cols] / run_sum[:, cols]).T
        out_ref[:, h * HEAD_SIZE : (h + 1) * HEAD_SIZE] = attended.astype(BF16)


def remote(src, dst, send_sem, recv_sem, where):
    return pltpu.make_async_remote_copy(
        src_ref=src,
        dst_ref=dst,
        send_sem=send_sem,
        recv_sem=recv_sem,
        device_id=where,
        device_id_type=MESH,
    )


def layer_kernel(
    n_ep,
    n_tp,
    heads,
    send_ref,
    key_ref,
    value_ref,
    query_ref,
    query_gain_ref,
    forget_ref,
    gate_ref,
    up_ref,
    down_ref,
    out_ref,
    back_ref,
    heads_ref,
    out_all,
    rows_all,
    total,
    result,
    attended,
    keys_all,
    values_all,
    query_t,
    bias,
    run_max,
    run_sum,
    acc,
    gate_all,
    up_all,
    down_all,
    out_own,
    row_send,
    row_recv,
    fwd_send,
    fwd_recv,
    bwd_send,
    bwd_recv,
    core_send,
    core_recv,
    side_send,
    side_recv,
    half_send,
    half_recv,
    part_send,
    part_recv,
    back_send,
    back_recv,
    head_send,
    head_recv,
    local,
):
    me, t = lax.axis_index("ep"), lax.axis_index("tp")
    n_z = n_ep // CORES
    z, core = me // CORES, lax.rem(me, CORES)
    offset = lax.rem(t + (n_tp - 1) * me, n_tp)
    here = n_ep // n_tp
    right, left = lax.rem(t + 1, n_tp), lax.rem(t + n_tp - 1, n_tp)
    across = lax.rem(t + 2, n_tp)
    up_ep = CORES * lax.rem(z + 1, n_z) + core
    down_ep = CORES * lax.rem(z + n_z - 1, n_z) + core
    other = CORES * z + (1 - core)
    reach = n_z // 2
    self_slot = me // n_tp
    is_self = lax.rem(me, n_tp) == offset
    far_first = [here // 2]
    for k in range(1, here // 2):
        far_first += [here // 2 - k, here // 2 + k]
    far_first.append(0)

    barrier = pltpu.get_barrier_semaphore()
    for where in (
        {"ep": up_ep},
        {"ep": down_ep},
        {"ep": other},
        {"tp": right},
        {"tp": left},
        {"tp": across},
    ):
        pl.semaphore_signal(barrier, inc=1, device_id=where, device_id_type=MESH)
    for m in range(here):
        mate = offset + n_tp * m

        @pl.when(mate != me)
        def _(mate=mate):
            pl.semaphore_signal(barrier, inc=1, device_id={"ep": mate}, device_id_type=MESH)

    def returns_from(e):
        column = lax.rem(me + e, n_tp)
        return column, jnp.logical_not(jnp.logical_and(me == e, column == t))

    for e in range(n_ep):
        column, away = returns_from(e)

        @pl.when(away)
        def _(e=e, column=column):
            pl.semaphore_signal(
                barrier, inc=1, device_id={"ep": e, "tp": column}, device_id_type=MESH
            )

    pl.semaphore_wait(barrier, 6 + here + n_ep - jnp.where(is_self, 2, 0))

    weights = ((gate_ref, gate_all), (up_ref, up_all), (down_ref, down_all))
    out_rows = out_ref.shape[0] // CORES
    out_first = core * out_rows

    def side_copy(a, way):
        where = {"tp": (right, left)[way]}
        if a < 3:
            src, dst = weights[a][0], weights[a][1].at[t]
        else:
            mine = pl.ds(out_first, out_rows)
            src, dst = out_ref.at[mine], out_all.at[t, mine]
        return remote(src, dst, side_send.at[a, way], side_recv.at[a, way], where)

    def half_copy(a, way):
        where = {"tp": (right, left)[way]}
        owner = (left, right)[way]
        if a < 3:
            full = weights[a][1]
            half = full.shape[1] // 2
            part = full.at[owner, pl.ds(way * half, half)]
        else:
            half = out_rows // 2
            part = out_all.at[owner, pl.ds(out_first + way * half, half)]
        return remote(part, part, half_send.at[a, way], half_recv.at[a, way], where)

    def hand_on(a):
        for way in range(2):
            side_copy(a, way).wait_recv()
            half_copy(a, way).start()

    def part_copy(k, first):
        part = out_all.at[(left, right, across)[k], pl.ds(first, out_rows)]
        return remote(part, part, part_send.at[k], part_recv.at[k], {"ep": other})

    own = [
        pltpu.make_async_copy(src, full.at[t], local.at[a])
        for a, (src, full) in enumerate(weights)
    ]
    own_row = pltpu.make_async_copy(
        send_ref.at[self_slot], rows_all.at[self_slot], local.at[3]
    )
    own_out = (
        pltpu.make_async_copy(out_ref, out_own, local.at[4]),
        pltpu.make_async_copy(out_own, out_all.at[t], local.at[4]),
    )

    def row_copy(k):
        m = lax.rem(self_slot + k, here)
        mate = offset + n_tp * m
        return mate, remote(
            send_ref.at[m],
            rows_all.at[self_slot],
            row_send.at[m],
            row_recv.at[self_slot],
            {"ep": mate},
        )

    def row_arrival(n):
        source = offset + n_tp * n
        return source, remote(
            send_ref.at[n], rows_all.at[n], row_send.at[n], row_recv.at[n], {"ep": source}
        )

    def block_copy(part, source_z, source_core, send_sem, recv_sem, where, mine=False):
        block = (keys_all, values_all)[part].at[CORES * source_z + source_core]
        return remote((key_ref, value_ref)[part] if mine else block, block, send_sem, recv_sem, where)

    def fwd_copy(s, part):
        source = lax.rem(z - s + n_z, n_z)
        sems = fwd_send.at[s, part], fwd_recv.at[s, part]
        return block_copy(part, source, core, *sems, {"ep": up_ep}, s == 0)

    def fwd_arrival(s, part):
        source = lax.rem(z - 1 - s + n_z, n_z)
        sems = fwd_send.at[s, part], fwd_recv.at[s, part]
        return block_copy(part, source, core, *sems, {"ep": up_ep})

    def bwd_copy(s, part):
        sems = bwd_send.at[s, part], bwd_recv.at[s, part]
        return block_copy(part, lax.rem(z + s, n_z), core, *sems, {"ep": down_ep}, s == 0)

    def bwd_arrival(s, part):
        sems = bwd_send.at[s, part], bwd_recv.at[s, part]
        return block_copy(part, lax.rem(z + 1 + s, n_z), core, *sems, {"ep": down_ep})

    def core_copy(k, part, source_z, source_core, mine=False):
        sems = core_send.at[k, part], core_recv.at[k, part]
        return block_copy(part, source_z, source_core, *sems, {"ep": other}, mine)

    def core_fwd(s, part, source_core):
        return core_copy(1 + s, part, lax.rem(z - 1 - s + n_z, n_z), source_core)

    def core_bwd(s, part, source_core):
        return core_copy(1 + reach + s, part, lax.rem(z + 1 + s, n_z), source_core)

    def fwd_sends(s):
        return jnp.logical_and(z - s >= 0, z + 1 <= n_z - 1)

    def fwd_gets(s):
        return z - 1 - s >= 0

    def bwd_sends(s):
        return lax.rem(z + s, n_z) <= reach - 2

    def bwd_gets(s):
        return lax.rem(z + 1 + s, n_z) <= reach - 2

    def bwd_needed(s):
        return jnp.logical_and(bwd_gets(s), lax.rem(z + 1 + s, n_z) < z)

    def back_copy(k, j):
        n = lax.rem(self_slot + far_first[k], here)
        q = lax.rem(t + j, n_tp)
        target = offset + n_tp * n
        away = jnp.logical_not(jnp.logical_and(target == me, q == t))
        return away, remote(
            result.at[q, n],
            back_ref.at[me],
            back_send.at[k, j],
            back_recv.at[me],
            {"ep": target, "tp": q},
        )

    own_back = pltpu.make_async_copy(result.at[t, self_slot], back_ref.at[me], local.at[3])

    token_rows = attended.shape[0] // n_tp

    def head_copy(k):
        q = lax.rem(t + k, n_tp)
        first = pl.multiple_of(q * token_rows, token_rows)
        return remote(
            attended.at[pl.ds(first, token_rows)],
            heads_ref.at[t],
            head_send.at[k],
            head_recv.at[k],
            {"tp": q},
        )

    own_heads = pltpu.make_async_copy(
        attended.at[pl.ds(pl.multiple_of(t * token_rows, token_rows), token_rows)],
        heads_ref.at[t],
        local.at[0],
    )

    def expert_part(p, first):
        rows = rows_all[...].reshape(here * CAP, rows_all.shape[2])
        gate = dot(rows, gate_all[p])
        up = dot(rows, up_all[p])
        hidden = (gate / (1.0 + jnp.exp(-gate)) * up).astype(BF16)
        width = result.shape[3]
        for q in range(n_tp):
            cols = slice(q * width, (q + 1) * width)
            piece = dot(hidden, down_all[p, :, cols]).astype(BF16).astype(F32)
            if first:
                total[:, cols] = piece
            else:
                total[:, cols] += piece

    for a in range(3):
        for way in range(2):
            side_copy(a, way).start()

    for k in far_first:
        mate, copy = row_copy(k)

        @pl.when(mate != me)
        def _(copy=copy):
            copy.start()

    for part in range(2):

        @pl.when(fwd_sends(0))
        def _(part=part):
            fwd_copy(0, part).start()

        @pl.when(bwd_sends(0))
        def _(part=part):
            bwd_copy(0, part).start()

        @pl.when(core == 0)
        def _(part=part):
            core_copy(0, part, z, 0, True).start()

    for copy in own:
        copy.start()
    own_out[0].start()

    @pl.when(is_self)
    def _():
        own_row.start()

    keys_all[me] = key_ref[...]
    values_all[me] = value_ref[...]
    prepare_attention(
        heads, me + 1, query_ref, query_gain_ref, forget_ref, query_t, bias, run_max, run_sum, acc
    )
    own_out[0].wait()
    own_out[1].start()
    for copy in own:
        copy.wait()

    hand_on(0)
    for s in range(reach):
        for part in range(2):

            @pl.when(fwd_gets(s))
            def _(s=s, part=part):
                fwd_arrival(s, part).wait_recv()

            if s + 1 < reach:

                @pl.when(fwd_sends(s + 1))
                def _(s=s, part=part):
                    fwd_copy(s + 1, part).start()

            @pl.when(fwd_gets(s))
            def _(s=s, part=part):
                core_fwd(s, part, core).start()

            if s < reach - 1:

                @pl.when(bwd_gets(s))
                def _(s=s, part=part):
                    bwd_arrival(s, part).wait_recv()

                if s + 1 < reach - 1:

                    @pl.when(bwd_sends(s + 1))
                    def _(s=s, part=part):
                        bwd_copy(s + 1, part).start()

                @pl.when(bwd_needed(s))
                def _(s=s, part=part):
                    core_bwd(s, part, core).start()

        if s == 0:
            hand_on(1)
        if s == 2:
            hand_on(2)
            for way in range(2):
                side_copy(3, way).start()
            for n in range(here):
                source, arrival = row_arrival(n)

                @pl.when(source != me)
                def _(arrival=arrival):
                    arrival.wait_recv()

            @pl.when(is_self)
            def _():
                own_row.wait()

            expert_part(t, True)
        if s == 3:
            expert_part(left, False)
        if s == 4:
            expert_part(right, False)

    hand_on(3)
    for a in range(3):
        for way in range(2):
            half_copy(a, way).wait_recv()
    expert_part(across, False)
    width = result.shape[3]
    for k in far_first:
        n = lax.rem(self_slot + k, here)
        first = pl.multiple_of(n * CAP, CAP)
        for q in range(n_tp):
            result[q, n] = total[pl.ds(first, CAP), q * width : (q + 1) * width].astype(BF16)
    for k in range(here):
        for j in range(n_tp):
            away, copy = back_copy(k, j)

            @pl.when(away)
            def _(copy=copy):
                copy.start()

    @pl.when(is_self)
    def _():
        own_back.start()

    for part in range(2):

        @pl.when(core == 1)
        def _(part=part):
            core_copy(0, part, z, 0).wait_recv()

        for s in range(reach):

            @pl.when(fwd_gets(s))
            def _(s=s, part=part):
                core_fwd(s, part, 1 - core).wait_recv()

            if s < reach - 1:

                @pl.when(bwd_needed(s))
                def _(s=s, part=part):
                    core_bwd(s, part, 1 - core).wait_recv()

    state = (keys_all, values_all, query_t, bias, run_max, run_sum, acc)

    def body(block, carry):
        attend_block(block, False, *state)
        return carry

    for way in range(2):
        part_copy(way, out_first).start()
    lax.fori_loop(0, me, body, 0)
    attend_block(me, True, *state)
    finish_attention(heads, attended, run_sum, acc)
    for way in range(2):
        half_copy(3, way).wait_recv()
    part_copy(2, out_first).start()
    for k in range(1, n_tp):
        head_copy(k).start()
    own_heads.start()

    for a in range(4):
        for way in range(2):
            side_copy(a, way).wait_send()
            half_copy(a, way).wait_send()
    for k in range(here):
        mate, copy = row_copy(k)

        @pl.when(mate != me)
        def _(copy=copy):
            copy.wait_send()

    for part in range(2):

        @pl.when(core == 0)
        def _(part=part):
            core_copy(0, part, z, 0, True).wait_send()

        for s in range(reach):

            @pl.when(fwd_sends(s))
            def _(s=s, part=part):
                fwd_copy(s, part).wait_send()

            @pl.when(fwd_gets(s))
            def _(s=s, part=part):
                core_fwd(s, part, core).wait_send()

            if s < reach - 1:

                @pl.when(bwd_sends(s))
                def _(s=s, part=part):
                    bwd_copy(s, part).wait_send()

                @pl.when(bwd_needed(s))
                def _(s=s, part=part):
                    core_bwd(s, part, core).wait_send()

    for k in range(3):
        part_copy(k, out_first).wait_send()
        part_copy(k, (1 - core) * out_rows).wait_recv()
    own_out[1].wait()
    for k in range(here):
        for j in range(n_tp):
            away, copy = back_copy(k, j)

            @pl.when(away)
            def _(copy=copy):
                copy.wait_send()

    for e in range(n_ep):
        column, away = returns_from(e)
        arrival = remote(
            result.at[0, 0],
            back_ref.at[e],
            back_send.at[0, 0],
            back_recv.at[e],
            {"ep": e, "tp": column},
        )

        @pl.when(away)
        def _(arrival=arrival):
            arrival.wait_recv()

    @pl.when(is_self)
    def _():
        own_back.wait()

    for k in range(1, n_tp):
        source = lax.rem(t + n_tp - k, n_tp)
        head_copy(k).wait_send()
        remote(
            attended.at[pl.ds(0, token_rows)],
            heads_ref.at[source],
            head_send.at[k],
            head_recv.at[k],
            {"tp": source},
        ).wait_recv()
    own_heads.wait()


def combine_kernel(back_ref, routes_ref, weight_ref, heads_ref, out_w_ref, mixer_ref, out_ref):
    slots = back_ref.shape[0]
    span = routes_ref.shape[1]
    expert_col = lax.broadcasted_iota(jnp.int32, (EXPERTS, 1), 0)
    routes = routes_ref[...]
    _, rank = member_and_rank(routes, expert_col)
    total = None
    for j in range(TOP):
        chosen = routes[j : j + 1, :]
        within = jnp.sum(jnp.where(chosen == expert_col, rank, 0.0), axis=0, keepdims=True)
        slot = chosen * CAP + within.astype(jnp.int32)
        at = lax.broadcasted_iota(jnp.int32, (slots, span), 0)
        pick = jnp.where(at == slot, 1.0, 0.0).astype(BF16)
        picked = dot(pick, back_ref[...], (((0,), (0,)), ((), ())))
        term = picked * weight_ref[:, j : j + 1]
        total = term if total is None else total + term
    out_ref[...] = total.astype(BF16)
    projected = None
    for k in range(heads_ref.shape[0]):
        piece = dot(heads_ref[k], out_w_ref[k])
        projected = piece if projected is None else projected + piece
    mixer_ref[...] = projected.astype(BF16)


def on_device(
    n_ep,
    n_tp,
    queries,
    key_rows,
    value_rows,
    query_gain,
    key_gain,
    log_forget,
    out_weight,
    expert_rows,
    expert_gain,
    routes,
    route_weight,
    gate_weight,
    up_weight,
    down_weight,
):
    span, model_width = expert_rows.shape
    here = n_ep // n_tp
    heads = queries.shape[1] // HEAD_SIZE
    width = model_width // n_tp
    n_z = n_ep // CORES
    reach = n_z // 2
    ff_part = gate_weight.shape[2]
    hbm = pl.BlockSpec(memory_space=pltpu.HBM)
    vmem = pl.BlockSpec(memory_space=pltpu.VMEM)
    shape = jax.ShapeDtypeStruct
    big = pltpu.CompilerParams(vmem_limit_bytes=56 * 1024 * 1024)

    send_rows, own_keys, own_values = pl.pallas_call(
        functools.partial(prologue_kernel, n_tp),
        out_shape=(
            shape((here, CAP, model_width), BF16),
            shape((span, HEAD_SIZE), BF16),
            shape((HEAD_SIZE, span), BF16),
        ),
        in_specs=[vmem] * 6,
        out_specs=(vmem,) * 3,
        scratch_shapes=[pltpu.VMEM((span, model_width), BF16)],
        compiler_params=big,
        name="prologue",
    )(
        expert_rows,
        expert_gain.reshape(1, -1),
        routes,
        key_rows,
        value_rows,
        key_gain.reshape(1, -1),
    )

    dma = pltpu.SemaphoreType.DMA
    columns = heads * span
    back_rows, head_rows, out_all = pl.pallas_call(
        functools.partial(layer_kernel, n_ep, n_tp, heads),
        out_shape=(
            shape((n_ep, CAP, width), BF16),
            shape((n_tp, span // n_tp, heads * HEAD_SIZE), BF16),
            shape((n_tp, *out_weight.shape), BF16),
        ),
        in_specs=[hbm] + [vmem] * 5 + [hbm] * 4,
        out_specs=(hbm,) * 3,
        scratch_shapes=[
            pltpu.VMEM((here, CAP, model_width), BF16),
            pltpu.VMEM((here * CAP, model_width), F32),
            pltpu.VMEM((n_tp, here, CAP, width), BF16),
            pltpu.VMEM((span, heads * HEAD_SIZE), BF16),
            pltpu.VMEM((n_ep, span, HEAD_SIZE), BF16),
            pltpu.VMEM((n_ep, HEAD_SIZE, span), BF16),
            pltpu.VMEM((2 * HEAD_SIZE, columns), BF16),
            pltpu.VMEM((n_ep, span, HEAD_SIZE), BF16),
            pltpu.VMEM((1, columns), F32),
            pltpu.VMEM((1, columns), F32),
            pltpu.VMEM((HEAD_SIZE, columns), F32),
            pltpu.VMEM((n_tp, model_width, ff_part), BF16),
            pltpu.VMEM((n_tp, model_width, ff_part), BF16),
            pltpu.VMEM((n_tp, ff_part, model_width), BF16),
            pltpu.VMEM(out_weight.shape, BF16),
            dma((here,)),
            dma((here,)),
            dma((reach, 2)),
            dma((reach, 2)),
            dma((reach - 1, 2)),
            dma((reach - 1, 2)),
            dma((2 * reach, 2)),
            dma((2 * reach, 2)),
            dma((4, 2)),
            dma((4, 2)),
            dma((4, 2)),
            dma((4, 2)),
            dma((3,)),
            dma((3,)),
            dma((here, n_tp)),
            dma((n_ep,)),
            dma((n_tp,)),
            dma((n_tp,)),
            dma((5,)),
        ],
        compiler_params=pltpu.CompilerParams(
            collective_id=0, has_side_effects=True, vmem_limit_bytes=60 * 1024 * 1024
        ),
        name="layer",
    )(
        send_rows,
        own_keys,
        own_values,
        queries,
        query_gain.reshape(1, -1),
        log_forget,
        gate_weight.reshape(model_width, ff_part),
        up_weight.reshape(model_width, ff_part),
        down_weight.reshape(ff_part, model_width),
        out_weight,
    )

    mixer_out, expert_out = pl.pallas_call(
        combine_kernel,
        out_shape=(
            shape((span // n_tp, model_width), BF16),
            shape((span, width), BF16),
        ),
        in_specs=[vmem] * 5,
        out_specs=(vmem, vmem),
        compiler_params=big,
        name="combine",
    )(back_rows.reshape(n_ep * CAP, width), routes, route_weight.T, head_rows, out_all)
    return (mixer_out, expert_out)


def solution(mesh):
    in_specs = (
        P(("grp", "ep"), "tp"),
        P(("grp", "ep"), "tp"),
        P(("grp", "ep"), "tp"),
        P(),
        P(),
        P("tp", "grp"),
        P("tp", None),
        P(("grp", "ep"), None),
        P(),
        P(None, ("grp", "ep")),
        P(None, ("grp", "ep")),
        P("ep", None, "tp"),
        P("ep", None, "tp"),
        P("ep", "tp", None),
    )
    out_specs = (P(("grp", "ep", "tp"), None), P(("grp", "ep"), "tp"))
    return jax.shard_map(
        functools.partial(on_device, mesh.shape["ep"], mesh.shape["tp"]),
        mesh=mesh,
        in_specs=in_specs,
        out_specs=out_specs,
        check_vma=False,
    )
```

```python
import functools

import jax
import jax.numpy as jnp
from jax import lax
from jax.experimental import pallas as pl
from jax.experimental.pallas import tpu as pltpu
from jax.sharding import PartitionSpec as P

HEAD_SIZE = 128
EXPERTS = 32
CAP = 48
TOP = 2
CORES = 2
LOG2E = 1.4426950408889634
MESH = pl.DeviceIdType.MESH
F32 = jnp.float32
BF16 = jnp.bfloat16


def dot(a, b, dims=(((1,), (0,)), ((), ()))):
    return lax.dot_general(a, b, dims, preferred_element_type=F32)


def row_norm(rows, gain):
    wide = rows.astype(F32)
    factor = lax.rsqrt(jnp.mean(wide * wide, axis=-1, keepdims=True) + 1e-06)
    return wide * factor * gain


def member_and_rank(routes, expert_col):
    tokens = routes.shape[1]
    named = jnp.logical_or(routes[0:1, :] == expert_col, routes[1:2, :] == expert_col)
    member = jnp.where(named, 1.0, 0.0).astype(F32)
    before = lax.broadcasted_iota(jnp.int32, (tokens, tokens), 0)
    after = lax.broadcasted_iota(jnp.int32, (tokens, tokens), 1)
    earlier = jnp.where(before < after, 1.0, 0.0).astype(BF16)
    return member, dot(member.astype(BF16), earlier)


def gather_rows(n_tp, offset, rows_ref, gain_ref, routes_ref, send, normed):
    span = rows_ref.shape[0]
    step = 64
    for first in range(0, span, step):
        normed[first : first + step, :] = row_norm(
            rows_ref[first : first + step, :], gain_ref[...]
        ).astype(BF16)
    here = EXPERTS // n_tp
    expert_col = offset + n_tp * lax.broadcasted_iota(jnp.int32, (here, 1), 0)
    member, rank = member_and_rank(routes_ref[...], expert_col)
    place = jnp.where(member > 0.5, rank, -1.0)
    slot = lax.broadcasted_iota(jnp.int32, (CAP, span), 0).astype(F32)
    for m in range(here):
        pick = jnp.where(place[m : m + 1, :] == slot, 1.0, 0.0).astype(BF16)
        send[m] = dot(pick, normed[...]).astype(BF16)


def token_columns(routes, weights):
    expert_col = lax.broadcasted_iota(jnp.int32, (EXPERTS, 1), 0)
    _, rank = member_and_rank(routes, expert_col)
    rows = []
    for j in range(TOP):
        chosen = routes[j : j + 1, :]
        within = jnp.sum(jnp.where(chosen == expert_col, rank, 0.0), axis=0, keepdims=True)
        rows.append((chosen * CAP).astype(F32) + within)
    rows.append(weights)
    rows.append(jnp.zeros((8 - 2 * TOP, routes.shape[1]), F32))
    return jnp.concatenate(rows, axis=0).T


def split_three(value):
    high = value.astype(BF16)
    rest = value - high.astype(F32)
    mid = rest.astype(BF16)
    low = (rest - mid.astype(F32)).astype(BF16)
    return high.astype(F32), mid.astype(F32), low.astype(F32)


def prepare_attention(
    heads, blocks, query_ref, gain_ref, forget_ref, query_t, bias, run_max, run_sum, acc
):
    span = query_ref.shape[0]
    columns = heads * span
    for h in range(heads):
        normed = row_norm(query_ref[:, h * HEAD_SIZE : (h + 1) * HEAD_SIZE], gain_ref[...])
        rounded = normed.astype(BF16).astype(F32)
        query_t[:HEAD_SIZE, h * span : (h + 1) * span] = rounded.T.astype(BF16)
    row = lax.broadcasted_iota(jnp.int32, (HEAD_SIZE, columns), 0)
    head = lax.broadcasted_iota(jnp.int32, (HEAD_SIZE, columns), 1) // span
    query_t[HEAD_SIZE:, :] = jnp.where(row // 3 == head, 1.0, 0.0).astype(BF16)
    run_max[...] = jnp.full(run_max.shape, -1e30, F32)
    run_sum[...] = jnp.zeros(run_sum.shape, F32)
    acc[...] = jnp.zeros(acc.shape, F32)
    lane = lax.broadcasted_iota(jnp.int32, (8, HEAD_SIZE), 1)
    sub = lax.broadcasted_iota(jnp.int32, (8, HEAD_SIZE), 0)
    place = jnp.where(lane == sub, 1.0, 0.0).astype(BF16)

    def one(block, carry):
        first = pl.multiple_of(block * span, span)
        rows = []
        for h in range(heads):
            gates = forget_ref[h : h + 1, pl.ds(first, span)]
            rows.extend(split_three(gates * (-(HEAD_SIZE**0.5))))
        rows.append(jnp.zeros((8 - len(rows), span), F32))
        stacked = jnp.concatenate(rows, axis=0).astype(BF16)
        bias[block] = dot(stacked, place, (((0,), (0,)), ((), ()))).astype(BF16)
        return carry

    lax.fori_loop(0, blocks, one, 0)


def attend_block(block, masked, keys_all, values_all, query_t, bias, run_max, run_sum, acc):
    span = keys_all.shape[1]
    columns = query_t.shape[1]
    exp_scale = HEAD_SIZE ** (-0.5) * LOG2E
    width = 256
    keys = jnp.concatenate([keys_all[block], bias[block]], axis=1)
    values = values_all[block]
    for first_col in range(0, columns, width):
        cols = slice(first_col, first_col + width)
        scores = dot(keys, query_t[:, cols])
        if masked:
            key_at = lax.broadcasted_iota(jnp.int32, (span, width), 0)
            query_at = lax.broadcasted_iota(jnp.int32, (span, width), 1) + first_col % span
            scores = jnp.where(key_at <= query_at, scores, -1e30)
        old_max = run_max[:, cols]
        new_max = jnp.maximum(old_max, jnp.max(scores, axis=0, keepdims=True))
        shrink = jnp.exp2((old_max - new_max) * exp_scale)
        weights = jnp.exp2((scores - new_max) * exp_scale)
        run_max[:, cols] = new_max
        run_sum[:, cols] = shrink * run_sum[:, cols] + jnp.sum(weights, axis=0, keepdims=True)
        acc[:, cols] = shrink * acc[:, cols] + dot(values, weights.astype(BF16))


def finish_attention(heads, out_ref, run_sum, acc):
    span = out_ref.shape[0]
    for h in range(heads):
        cols = slice(h * span, (h + 1) * span)
        attended = (acc[:, cols] / run_sum[:, cols]).T
        out_ref[:, h * HEAD_SIZE : (h + 1) * HEAD_SIZE] = attended.astype(BF16)


def remote(src, dst, send_sem, recv_sem, where):
    return pltpu.make_async_remote_copy(
        src_ref=src,
        dst_ref=dst,
        send_sem=send_sem,
        recv_sem=recv_sem,
        device_id=where,
        device_id_type=MESH,
    )


def layer_kernel(
    n_ep,
    n_tp,
    heads,
    rows_ref,
    rows_gain_ref,
    routes_ref,
    route_weight_ref,
    raw_key_ref,
    raw_value_ref,
    key_gain_ref,
    query_ref,
    query_gain_ref,
    forget_ref,
    gate_ref,
    up_ref,
    down_ref,
    out_ref,
    mixer_ref,
    expert_ref,
    send_ref,
    normed,
    columns_ref,
    picks,
    back_ref,
    heads_ref,
    out_all,
    key_ref,
    value_ref,
    rows_all,
    total,
    result,
    attended,
    keys_all,
    values_all,
    query_t,
    bias,
    run_max,
    run_sum,
    acc,
    gate_all,
    up_all,
    down_all,
    row_send,
    row_recv,
    fwd_send,
    fwd_recv,
    bwd_send,
    bwd_recv,
    core_send,
    core_recv,
    side_send,
    side_recv,
    half_send,
    half_recv,
    part_send,
    part_recv,
    back_send,
    back_recv,
    head_send,
    head_recv,
    local,
):
    me, t = lax.axis_index("ep"), lax.axis_index("tp")
    n_z = n_ep // CORES
    z, core = me // CORES, lax.rem(me, CORES)
    offset = lax.rem(t + (n_tp - 1) * me, n_tp)
    here = n_ep // n_tp
    right, left = lax.rem(t + 1, n_tp), lax.rem(t + n_tp - 1, n_tp)
    across = lax.rem(t + 2, n_tp)
    up_ep = CORES * lax.rem(z + 1, n_z) + core
    down_ep = CORES * lax.rem(z + n_z - 1, n_z) + core
    other = CORES * z + (1 - core)
    reach = n_z // 2
    self_slot = me // n_tp
    is_self = lax.rem(me, n_tp) == offset
    far_first = [here // 2]
    for k in range(1, here // 2):
        far_first += [here // 2 - k, here // 2 + k]
    far_first.append(0)

    barrier = pltpu.get_barrier_semaphore()
    for where in (
        {"ep": up_ep},
        {"ep": down_ep},
        {"ep": other},
        {"tp": right},
        {"tp": left},
        {"tp": across},
    ):
        pl.semaphore_signal(barrier, inc=1, device_id=where, device_id_type=MESH)
    for m in range(here):
        mate = offset + n_tp * m

        @pl.when(mate != me)
        def _(mate=mate):
            pl.semaphore_signal(barrier, inc=1, device_id={"ep": mate}, device_id_type=MESH)

    def returns_from(e):
        column = lax.rem(me + e, n_tp)
        return column, jnp.logical_not(jnp.logical_and(me == e, column == t))

    for e in range(n_ep):
        column, away = returns_from(e)

        @pl.when(away)
        def _(e=e, column=column):
            pl.semaphore_signal(
                barrier, inc=1, device_id={"ep": e, "tp": column}, device_id_type=MESH
            )

    pl.semaphore_wait(barrier, 6 + here + n_ep - jnp.where(is_self, 2, 0))

    weights = ((gate_ref, gate_all), (up_ref, up_all), (down_ref, down_all))
    out_rows = out_ref.shape[0] // CORES
    out_first = core * out_rows

    def side_copy(a, way):
        where = {"tp": (right, left)[way]}
        if a < 3:
            src, dst = weights[a][0], weights[a][1].at[t]
        else:
            mine = pl.ds(out_first, out_rows)
            src, dst = out_ref.at[mine], out_all.at[t, mine]
        return remote(src, dst, side_send.at[a, way], side_recv.at[a, way], where)

    def half_copy(a, way):
        where = {"tp": (right, left)[way]}
        owner = (left, right)[way]
        if a < 3:
            full = weights[a][1]
            half = full.shape[1] // 2
            part = full.at[owner, pl.ds(way * half, half)]
        else:
            half = out_rows // 2
            part = out_all.at[owner, pl.ds(out_first + way * half, half)]
        return remote(part, part, half_send.at[a, way], half_recv.at[a, way], where)

    def hand_on(a):
        for way in range(2):
            side_copy(a, way).wait_recv()
            half_copy(a, way).start()

    def part_copy(k, first):
        part = out_all.at[(left, right, across)[k], pl.ds(first, out_rows)]
        return remote(part, part, part_send.at[k], part_recv.at[k], {"ep": other})

    own = [
        pltpu.make_async_copy(src, full.at[t], local.at[a])
        for a, (src, full) in enumerate(weights)
    ]
    own_out = pltpu.make_async_copy(out_ref, out_all.at[t], local.at[3])

    def row_copy(k):
        m = lax.rem(self_slot + k, here)
        mate = offset + n_tp * m
        return mate, remote(
            send_ref.at[m],
            rows_all.at[self_slot],
            row_send.at[m],
            row_recv.at[self_slot],
            {"ep": mate},
        )

    def row_arrival(n):
        source = offset + n_tp * n
        return source, remote(
            send_ref.at[n], rows_all.at[n], row_send.at[n], row_recv.at[n], {"ep": source}
        )

    def block_copy(part, source_z, source_core, send_sem, recv_sem, where, mine=False):
        block = (keys_all, values_all)[part].at[CORES * source_z + source_core]
        return remote((key_ref, value_ref)[part] if mine else block, block, send_sem, recv_sem, where)

    def fwd_copy(s, part):
        source = lax.rem(z - s + n_z, n_z)
        sems = fwd_send.at[s, part], fwd_recv.at[s, part]
        return block_copy(part, source, core, *sems, {"ep": up_ep}, s == 0)

    def fwd_arrival(s, part):
        source = lax.rem(z - 1 - s + n_z, n_z)
        sems = fwd_send.at[s, part], fwd_recv.at[s, part]
        return block_copy(part, source, core, *sems, {"ep": up_ep})

    def bwd_copy(s, part):
        sems = bwd_send.at[s, part], bwd_recv.at[s, part]
        return block_copy(part, lax.rem(z + s, n_z), core, *sems, {"ep": down_ep}, s == 0)

    def bwd_arrival(s, part):
        sems = bwd_send.at[s, part], bwd_recv.at[s, part]
        return block_copy(part, lax.rem(z + 1 + s, n_z), core, *sems, {"ep": down_ep})

    def core_copy(k, part, source_z, source_core, mine=False):
        sems = core_send.at[k, part], core_recv.at[k, part]
        return block_copy(part, source_z, source_core, *sems, {"ep": other}, mine)

    def core_fwd(s, part, source_core):
        return core_copy(1 + s, part, lax.rem(z - 1 - s + n_z, n_z), source_core)

    def core_bwd(s, part, source_core):
        return core_copy(1 + reach + s, part, lax.rem(z + 1 + s, n_z), source_core)

    def fwd_sends(s):
        return jnp.logical_and(z - s >= 0, z + 1 <= n_z - 1)

    def fwd_gets(s):
        return z - 1 - s >= 0

    def bwd_sends(s):
        return lax.rem(z + s, n_z) <= reach - 2

    def bwd_gets(s):
        return lax.rem(z + 1 + s, n_z) <= reach - 2

    def bwd_needed(s):
        return jnp.logical_and(bwd_gets(s), lax.rem(z + 1 + s, n_z) < z)

    def back_copy(k, j):
        n = lax.rem(self_slot + far_first[k], here)
        q = lax.rem(t + j, n_tp)
        target = offset + n_tp * n
        away = jnp.logical_not(jnp.logical_and(target == me, q == t))
        return away, remote(
            result.at[q, n],
            back_ref.at[me],
            back_send.at[k, j],
            back_recv.at[me],
            {"ep": target, "tp": q},
        )

    token_rows = attended.shape[0] // n_tp

    def head_copy(k):
        q = lax.rem(t + k, n_tp)
        first = pl.multiple_of(q * token_rows, token_rows)
        return remote(
            attended.at[pl.ds(first, token_rows)],
            heads_ref.at[t],
            head_send.at[k],
            head_recv.at[k],
            {"tp": q},
        )

    def expert_part(p, first):
        rows = rows_all[...].reshape(here * CAP, rows_all.shape[2])
        gate = dot(rows, gate_all[p])
        up = dot(rows, up_all[p])
        hidden = (gate / (1.0 + jnp.exp(-gate)) * up).astype(BF16)
        width = result.shape[3]
        for q in range(n_tp):
            cols = slice(q * width, (q + 1) * width)
            piece = dot(hidden, down_all[p, :, cols]).astype(BF16).astype(F32)
            if first:
                total[:, cols] = piece
            else:
                total[:, cols] += piece

    for a in range(3):
        for way in range(2):
            side_copy(a, way).start()

    key_ref[...] = row_norm(raw_key_ref[...], key_gain_ref[...]).astype(BF16)
    value_ref[...] = raw_value_ref[...].astype(F32).T.astype(BF16)
    keys_all[me] = key_ref[...]
    values_all[me] = value_ref[...]
    for copy in own:
        copy.start()
    own_out.start()
    for part in range(2):

        @pl.when(fwd_sends(0))
        def _(part=part):
            fwd_copy(0, part).start()

        @pl.when(bwd_sends(0))
        def _(part=part):
            bwd_copy(0, part).start()

        @pl.when(core == 0)
        def _(part=part):
            core_copy(0, part, z, 0, True).start()

    gather_rows(n_tp, offset, rows_ref, rows_gain_ref, routes_ref, send_ref, normed)
    columns_ref[...] = token_columns(routes_ref[...], route_weight_ref[...])
    for k in far_first:
        mate, copy = row_copy(k)

        @pl.when(mate != me)
        def _(copy=copy):
            copy.start()

    @pl.when(is_self)
    def _():
        rows_all[self_slot] = send_ref[self_slot]

    prepare_attention(
        heads, me + 1, query_ref, query_gain_ref, forget_ref, query_t, bias, run_max, run_sum, acc
    )
    for copy in own:
        copy.wait()

    hand_on(0)
    for s in range(reach):
        for part in range(2):

            @pl.when(fwd_gets(s))
            def _(s=s, part=part):
                fwd_arrival(s, part).wait_recv()

            if s + 1 < reach:

                @pl.when(fwd_sends(s + 1))
                def _(s=s, part=part):
                    fwd_copy(s + 1, part).start()

            @pl.when(fwd_gets(s))
            def _(s=s, part=part):
                core_fwd(s, part, core).start()

            if s < reach - 1:

                @pl.when(bwd_gets(s))
                def _(s=s, part=part):
                    bwd_arrival(s, part).wait_recv()

                if s + 1 < reach - 1:

                    @pl.when(bwd_sends(s + 1))
                    def _(s=s, part=part):
                        bwd_copy(s + 1, part).start()

                @pl.when(bwd_needed(s))
                def _(s=s, part=part):
                    core_bwd(s, part, core).start()

        if s == 0:
            hand_on(1)
        if s == 2:
            hand_on(2)
            for way in range(2):
                side_copy(3, way).start()
        if s == 3:
            for n in range(here):
                source, arrival = row_arrival(n)

                @pl.when(source != me)
                def _(arrival=arrival):
                    arrival.wait_recv()

            expert_part(t, True)
        if s == 4:
            expert_part(left, False)
        if s == 5:
            expert_part(right, False)
        if s == 6:
            for a in range(3):
                for way in range(2):
                    half_copy(a, way).wait_recv()
            expert_part(across, False)
            width = result.shape[3]
            for k in far_first:
                n = lax.rem(self_slot + k, here)
                first = pl.multiple_of(n * CAP, CAP)
                for q in range(n_tp):
                    result[q, n] = total[pl.ds(first, CAP), q * width : (q + 1) * width].astype(
                        BF16
                    )
            for k in range(here):
                for j in range(n_tp):
                    away, copy = back_copy(k, j)

                    @pl.when(away)
                    def _(copy=copy):
                        copy.start()

            @pl.when(is_self)
            def _():
                back_ref[me] = result[t, self_slot]

    hand_on(3)
    for part in range(2):

        @pl.when(core == 1)
        def _(part=part):
            core_copy(0, part, z, 0).wait_recv()

        for s in range(reach):

            @pl.when(fwd_gets(s))
            def _(s=s, part=part):
                core_fwd(s, part, 1 - core).wait_recv()

            if s < reach - 1:

                @pl.when(bwd_needed(s))
                def _(s=s, part=part):
                    core_bwd(s, part, 1 - core).wait_recv()

    state = (keys_all, values_all, query_t, bias, run_max, run_sum, acc)

    def body(block, carry):
        attend_block(block, False, *state)
        return carry

    for way in range(2):
        part_copy(way, out_first).start()
    lax.fori_loop(0, me, body, 0)
    attend_block(me, True, *state)
    finish_attention(heads, attended, run_sum, acc)
    for way in range(2):
        half_copy(3, way).wait_recv()
    part_copy(2, out_first).start()
    for k in range(1, n_tp):
        head_copy(k).start()
    own_first = pl.multiple_of(t * token_rows, token_rows)
    heads_ref[t] = attended[pl.ds(own_first, token_rows), :]
    slot = lax.broadcasted_iota(jnp.int32, (8, n_ep * CAP), 1).astype(F32)[:1]
    for j in range(TOP):
        picks[j] = jnp.where(columns_ref[:, j : j + 1] == slot, 1.0, 0.0).astype(BF16)

    for a in range(4):
        for way in range(2):
            side_copy(a, way).wait_send()
            half_copy(a, way).wait_send()
    for k in range(here):
        mate, copy = row_copy(k)

        @pl.when(mate != me)
        def _(copy=copy):
            copy.wait_send()

    for part in range(2):

        @pl.when(core == 0)
        def _(part=part):
            core_copy(0, part, z, 0, True).wait_send()

        for s in range(reach):

            @pl.when(fwd_sends(s))
            def _(s=s, part=part):
                fwd_copy(s, part).wait_send()

            @pl.when(fwd_gets(s))
            def _(s=s, part=part):
                core_fwd(s, part, core).wait_send()

            if s < reach - 1:

                @pl.when(bwd_sends(s))
                def _(s=s, part=part):
                    bwd_copy(s, part).wait_send()

                @pl.when(bwd_needed(s))
                def _(s=s, part=part):
                    core_bwd(s, part, core).wait_send()

    for k in range(3):
        part_copy(k, out_first).wait_send()
        part_copy(k, (1 - core) * out_rows).wait_recv()
    own_out.wait()
    for k in range(1, n_tp):
        source = lax.rem(t + n_tp - k, n_tp)
        head_copy(k).wait_send()
        remote(
            attended.at[pl.ds(0, token_rows)],
            heads_ref.at[source],
            head_send.at[k],
            head_recv.at[k],
            {"tp": source},
        ).wait_recv()
    projected = None
    for k in range(n_tp):
        piece = dot(heads_ref[k], out_all[k])
        projected = piece if projected is None else projected + piece
    mixer_ref[...] = projected.astype(BF16)

    for k in range(here):
        for j in range(n_tp):
            away, copy = back_copy(k, j)

            @pl.when(away)
            def _(copy=copy):
                copy.wait_send()

    for e in range(n_ep):
        column, away = returns_from(e)
        arrival = remote(
            result.at[0, 0],
            back_ref.at[e],
            back_send.at[0, 0],
            back_recv.at[e],
            {"ep": e, "tp": column},
        )

        @pl.when(away)
        def _(arrival=arrival):
            arrival.wait_recv()

    expert_out = None
    for j in range(TOP):
        picked = dot(picks[j], back_ref[...].reshape(n_ep * CAP, back_ref.shape[2]))
        term = picked * columns_ref[:, TOP + j : TOP + j + 1]
        expert_out = term if expert_out is None else expert_out + term
    expert_ref[...] = expert_out.astype(BF16)


def on_device(
    n_ep,
    n_tp,
    queries,
    key_rows,
    value_rows,
    query_gain,
    key_gain,
    log_forget,
    out_weight,
    expert_rows,
    expert_gain,
    routes,
    route_weight,
    gate_weight,
    up_weight,
    down_weight,
):
    span, model_width = expert_rows.shape
    here = n_ep // n_tp
    heads = queries.shape[1] // HEAD_SIZE
    width = model_width // n_tp
    n_z = n_ep // CORES
    reach = n_z // 2
    ff_part = gate_weight.shape[2]
    hbm = pl.BlockSpec(memory_space=pltpu.HBM)
    vmem = pl.BlockSpec(memory_space=pltpu.VMEM)
    shape = jax.ShapeDtypeStruct
    dma = pltpu.SemaphoreType.DMA
    columns = heads * span
    return pl.pallas_call(
        functools.partial(layer_kernel, n_ep, n_tp, heads),
        out_shape=(
            shape((span // n_tp, model_width), BF16),
            shape((span, width), BF16),
        ),
        in_specs=[vmem] * 10 + [hbm] * 4,
        out_specs=(vmem, vmem),
        scratch_shapes=[
            pltpu.VMEM((here, CAP, model_width), BF16),
            pltpu.VMEM((span, model_width), BF16),
            pltpu.VMEM((span, 8), F32),
            pltpu.VMEM((TOP, span, n_ep * CAP), BF16),
            pltpu.VMEM((n_ep, CAP, width), BF16),
            pltpu.VMEM((n_tp, span // n_tp, heads * HEAD_SIZE), BF16),
            pltpu.VMEM((n_tp, *out_weight.shape), BF16),
            pltpu.VMEM((span, HEAD_SIZE), BF16),
            pltpu.VMEM((HEAD_SIZE, span), BF16),
            pltpu.VMEM((here, CAP, model_width), BF16),
            pltpu.VMEM((here * CAP, model_width), F32),
            pltpu.VMEM((n_tp, here, CAP, width), BF16),
            pltpu.VMEM((span, heads * HEAD_SIZE), BF16),
            pltpu.VMEM((n_ep, span, HEAD_SIZE), BF16),
            pltpu.VMEM((n_ep, HEAD_SIZE, span), BF16),
            pltpu.VMEM((2 * HEAD_SIZE, columns), BF16),
            pltpu.VMEM((n_ep, span, HEAD_SIZE), BF16),
            pltpu.VMEM((1, columns), F32),
            pltpu.VMEM((1, columns), F32),
            pltpu.VMEM((HEAD_SIZE, columns), F32),
            pltpu.VMEM((n_tp, model_width, ff_part), BF16),
            pltpu.VMEM((n_tp, model_width, ff_part), BF16),
            pltpu.VMEM((n_tp, ff_part, model_width), BF16),
            dma((here,)),
            dma((here,)),
            dma((reach, 2)),
            dma((reach, 2)),
            dma((reach - 1, 2)),
            dma((reach - 1, 2)),
            dma((2 * reach, 2)),
            dma((2 * reach, 2)),
            dma((4, 2)),
            dma((4, 2)),
            dma((4, 2)),
            dma((4, 2)),
            dma((3,)),
            dma((3,)),
            dma((here, n_tp)),
            dma((n_ep,)),
            dma((n_tp,)),
            dma((n_tp,)),
            dma((4,)),
        ],
        compiler_params=pltpu.CompilerParams(
            collective_id=0, has_side_effects=True, vmem_limit_bytes=60 * 1024 * 1024
        ),
        name="layer",
    )(
        expert_rows,
        expert_gain.reshape(1, -1),
        routes,
        route_weight,
        key_rows,
        value_rows,
        key_gain.reshape(1, -1),
        queries,
        query_gain.reshape(1, -1),
        log_forget,
        gate_weight.reshape(model_width, ff_part),
        up_weight.reshape(model_width, ff_part),
        down_weight.reshape(ff_part, model_width),
        out_weight,
    )


def solution(mesh):
    in_specs = (
        P(("grp", "ep"), "tp"),
        P(("grp", "ep"), "tp"),
        P(("grp", "ep"), "tp"),
        P(),
        P(),
        P("tp", "grp"),
        P("tp", None),
        P(("grp", "ep"), None),
        P(),
        P(None, ("grp", "ep")),
        P(None, ("grp", "ep")),
        P("ep", None, "tp"),
        P("ep", None, "tp"),
        P("ep", "tp", None),
    )
    out_specs = (P(("grp", "ep", "tp"), None), P(("grp", "ep"), "tp"))
    return jax.shard_map(
        functools.partial(on_device, mesh.shape["ep"], mesh.shape["tp"]),
        mesh=mesh,
        in_specs=in_specs,
        out_specs=out_specs,
        check_vma=False,
    )
```

```python
import functools

import jax
import jax.numpy as jnp
from jax import lax
from jax.experimental import pallas as pl
from jax.experimental.pallas import tpu as pltpu
from jax.sharding import PartitionSpec as P

HEAD_SIZE = 128
EXPERTS = 32
CAP = 48
TOP = 2
CORES = 2
LOG2E = 1.4426950408889634
MESH = pl.DeviceIdType.MESH
F32 = jnp.float32
BF16 = jnp.bfloat16


def dot(a, b, dims=(((1,), (0,)), ((), ()))):
    return lax.dot_general(a, b, dims, preferred_element_type=F32)


def row_norm(rows, gain):
    wide = rows.astype(F32)
    factor = lax.rsqrt(jnp.mean(wide * wide, axis=-1, keepdims=True) + 1e-06)
    return wide * factor * gain


def member_and_rank(routes, expert_col):
    tokens = routes.shape[1]
    named = jnp.logical_or(routes[0:1, :] == expert_col, routes[1:2, :] == expert_col)
    member = jnp.where(named, 1.0, 0.0).astype(F32)
    before = lax.broadcasted_iota(jnp.int32, (tokens, tokens), 0)
    after = lax.broadcasted_iota(jnp.int32, (tokens, tokens), 1)
    earlier = jnp.where(before < after, 1.0, 0.0).astype(BF16)
    return member, dot(member.astype(BF16), earlier)


def gather_rows(n_tp, offset, rows_ref, gain_ref, routes_ref, send, normed):
    span = rows_ref.shape[0]
    step = 64
    for first in range(0, span, step):
        normed[first : first + step, :] = row_norm(
            rows_ref[first : first + step, :], gain_ref[...]
        ).astype(BF16)
    here = EXPERTS // n_tp
    expert_col = offset + n_tp * lax.broadcasted_iota(jnp.int32, (here, 1), 0)
    member, rank = member_and_rank(routes_ref[...], expert_col)
    place = jnp.where(member > 0.5, rank, -1.0)
    slot = lax.broadcasted_iota(jnp.int32, (CAP, span), 0).astype(F32)
    for m in range(here):
        pick = jnp.where(place[m : m + 1, :] == slot, 1.0, 0.0).astype(BF16)
        send[m] = dot(pick, normed[...]).astype(BF16)


def token_columns(routes, weights):
    expert_col = lax.broadcasted_iota(jnp.int32, (EXPERTS, 1), 0)
    _, rank = member_and_rank(routes, expert_col)
    rows = []
    for j in range(TOP):
        chosen = routes[j : j + 1, :]
        within = jnp.sum(jnp.where(chosen == expert_col, rank, 0.0), axis=0, keepdims=True)
        rows.append((chosen * CAP).astype(F32) + within)
    rows.append(weights)
    rows.append(jnp.zeros((8 - 2 * TOP, routes.shape[1]), F32))
    return jnp.concatenate(rows, axis=0).T


def split_three(value):
    high = value.astype(BF16)
    rest = value - high.astype(F32)
    mid = rest.astype(BF16)
    low = (rest - mid.astype(F32)).astype(BF16)
    return high.astype(F32), mid.astype(F32), low.astype(F32)


def prepare_attention(
    heads, blocks, query_ref, gain_ref, forget_ref, query_t, bias, run_max, run_sum, acc
):
    span = query_ref.shape[0]
    columns = heads * span
    for h in range(heads):
        normed = row_norm(query_ref[:, h * HEAD_SIZE : (h + 1) * HEAD_SIZE], gain_ref[...])
        rounded = normed.astype(BF16).astype(F32)
        query_t[:HEAD_SIZE, h * span : (h + 1) * span] = rounded.T.astype(BF16)
    row = lax.broadcasted_iota(jnp.int32, (HEAD_SIZE, columns), 0)
    head = lax.broadcasted_iota(jnp.int32, (HEAD_SIZE, columns), 1) // span
    query_t[HEAD_SIZE:, :] = jnp.where(row // 3 == head, 1.0, 0.0).astype(BF16)
    run_max[...] = jnp.full(run_max.shape, -1e30, F32)
    run_sum[...] = jnp.zeros(run_sum.shape, F32)
    acc[...] = jnp.zeros(acc.shape, F32)
    lane = lax.broadcasted_iota(jnp.int32, (8, HEAD_SIZE), 1)
    sub = lax.broadcasted_iota(jnp.int32, (8, HEAD_SIZE), 0)
    place = jnp.where(lane == sub, 1.0, 0.0).astype(BF16)

    def one(block, carry):
        first = pl.multiple_of(block * span, span)
        rows = []
        for h in range(heads):
            gates = forget_ref[h : h + 1, pl.ds(first, span)]
            rows.extend(split_three(gates * (-(HEAD_SIZE**0.5))))
        rows.append(jnp.zeros((8 - len(rows), span), F32))
        stacked = jnp.concatenate(rows, axis=0).astype(BF16)
        bias[block] = dot(stacked, place, (((0,), (0,)), ((), ()))).astype(BF16)
        return carry

    lax.fori_loop(0, blocks, one, 0)


def attend_block(block, masked, keys_all, values_all, query_t, bias, run_max, run_sum, acc):
    span = keys_all.shape[1]
    columns = query_t.shape[1]
    exp_scale = HEAD_SIZE ** (-0.5) * LOG2E
    width = 256
    keys = jnp.concatenate([keys_all[block], bias[block]], axis=1)
    values = values_all[block]
    for first_col in range(0, columns, width):
        cols = slice(first_col, first_col + width)
        scores = dot(keys, query_t[:, cols])
        if masked:
            key_at = lax.broadcasted_iota(jnp.int32, (span, width), 0)
            query_at = lax.broadcasted_iota(jnp.int32, (span, width), 1) + first_col % span
            scores = jnp.where(key_at <= query_at, scores, -1e30)
        old_max = run_max[:, cols]
        new_max = jnp.maximum(old_max, jnp.max(scores, axis=0, keepdims=True))
        shrink = jnp.exp2((old_max - new_max) * exp_scale)
        weights = jnp.exp2((scores - new_max) * exp_scale)
        run_max[:, cols] = new_max
        run_sum[:, cols] = shrink * run_sum[:, cols] + jnp.sum(weights, axis=0, keepdims=True)
        acc[:, cols] = shrink * acc[:, cols] + dot(values, weights.astype(BF16))


def finish_attention(heads, out_ref, run_sum, acc):
    span = out_ref.shape[0]
    for h in range(heads):
        cols = slice(h * span, (h + 1) * span)
        attended = (acc[:, cols] / run_sum[:, cols]).T
        out_ref[:, h * HEAD_SIZE : (h + 1) * HEAD_SIZE] = attended.astype(BF16)


def remote(src, dst, send_sem, recv_sem, where):
    return pltpu.make_async_remote_copy(
        src_ref=src,
        dst_ref=dst,
        send_sem=send_sem,
        recv_sem=recv_sem,
        device_id=where,
        device_id_type=MESH,
    )


def layer_kernel(
    n_ep,
    n_tp,
    heads,
    rows_ref,
    rows_gain_ref,
    routes_ref,
    route_weight_ref,
    raw_key_ref,
    raw_value_ref,
    key_gain_ref,
    query_ref,
    query_gain_ref,
    forget_ref,
    gate_ref,
    up_ref,
    down_ref,
    out_ref,
    mixer_ref,
    expert_ref,
    send_ref,
    normed,
    columns_ref,
    picks,
    back_ref,
    heads_ref,
    out_all,
    key_ref,
    value_ref,
    rows_all,
    total,
    result,
    attended,
    keys_all,
    values_all,
    query_t,
    bias,
    run_max,
    run_sum,
    acc,
    gate_all,
    up_all,
    down_all,
    row_send,
    row_recv,
    fwd_send,
    fwd_recv,
    bwd_send,
    bwd_recv,
    core_send,
    core_recv,
    side_send,
    side_recv,
    half_send,
    half_recv,
    part_send,
    part_recv,
    back_send,
    back_recv,
    head_send,
    head_recv,
    local,
):
    me, t = lax.axis_index("ep"), lax.axis_index("tp")
    n_z = n_ep // CORES
    z, core = me // CORES, lax.rem(me, CORES)
    offset = lax.rem(t + (n_tp - 1) * me, n_tp)
    here = n_ep // n_tp
    right, left = lax.rem(t + 1, n_tp), lax.rem(t + n_tp - 1, n_tp)
    across = lax.rem(t + 2, n_tp)
    up_ep = CORES * lax.rem(z + 1, n_z) + core
    down_ep = CORES * lax.rem(z + n_z - 1, n_z) + core
    other = CORES * z + (1 - core)
    reach = n_z // 2
    self_slot = me // n_tp
    is_self = lax.rem(me, n_tp) == offset
    far_first = [here // 2]
    for k in range(1, here // 2):
        far_first += [here // 2 - k, here // 2 + k]
    far_first.append(0)

    barrier = pltpu.get_barrier_semaphore()
    for where in (
        {"ep": up_ep},
        {"ep": down_ep},
        {"ep": other},
        {"tp": right},
        {"tp": left},
        {"tp": across},
    ):
        pl.semaphore_signal(barrier, inc=1, device_id=where, device_id_type=MESH)
    for m in range(here):
        mate = offset + n_tp * m

        @pl.when(mate != me)
        def _(mate=mate):
            pl.semaphore_signal(barrier, inc=1, device_id={"ep": mate}, device_id_type=MESH)

    def returns_from(e):
        column = lax.rem(me + e, n_tp)
        return column, jnp.logical_not(jnp.logical_and(me == e, column == t))

    for e in range(n_ep):
        column, away = returns_from(e)

        @pl.when(away)
        def _(e=e, column=column):
            pl.semaphore_signal(
                barrier, inc=1, device_id={"ep": e, "tp": column}, device_id_type=MESH
            )

    pl.semaphore_wait(barrier, 6 + here + n_ep - jnp.where(is_self, 2, 0))

    weights = ((gate_ref, gate_all), (up_ref, up_all), (down_ref, down_all))
    out_rows = out_ref.shape[0] // CORES
    out_first = core * out_rows

    def side_copy(a, way):
        where = {"tp": (right, left)[way]}
        if a < 3:
            src, dst = weights[a][0], weights[a][1].at[t]
        else:
            mine = pl.ds(out_first, out_rows)
            src, dst = out_ref.at[mine], out_all.at[t, mine]
        return remote(src, dst, side_send.at[a, way], side_recv.at[a, way], where)

    def half_copy(a, way):
        where = {"tp": (right, left)[way]}
        owner = (left, right)[way]
        if a < 3:
            full = weights[a][1]
            half = full.shape[1] // 2
            part = full.at[owner, pl.ds(way * half, half)]
        else:
            half = out_rows // 2
            part = out_all.at[owner, pl.ds(out_first + way * half, half)]
        return remote(part, part, half_send.at[a, way], half_recv.at[a, way], where)

    def hand_on(a):
        for way in range(2):
            side_copy(a, way).wait_recv()
            half_copy(a, way).start()

    def part_copy(k, first):
        part = out_all.at[(left, right, across)[k], pl.ds(first, out_rows)]
        return remote(part, part, part_send.at[k], part_recv.at[k], {"ep": other})

    own = [
        pltpu.make_async_copy(src, full.at[t], local.at[a])
        for a, (src, full) in enumerate(weights)
    ]
    own_out = pltpu.make_async_copy(out_ref, out_all.at[t], local.at[3])

    def row_copy(k):
        m = lax.rem(self_slot + k, here)
        mate = offset + n_tp * m
        return mate, remote(
            send_ref.at[m],
            rows_all.at[self_slot],
            row_send.at[m],
            row_recv.at[self_slot],
            {"ep": mate},
        )

    def row_arrival(n):
        source = offset + n_tp * n
        return source, remote(
            send_ref.at[n], rows_all.at[n], row_send.at[n], row_recv.at[n], {"ep": source}
        )

    def block_copy(part, source_z, source_core, send_sem, recv_sem, where, mine=False):
        block = (keys_all, values_all)[part].at[CORES * source_z + source_core]
        return remote((key_ref, value_ref)[part] if mine else block, block, send_sem, recv_sem, where)

    def fwd_copy(s, part):
        source = lax.rem(z - s + n_z, n_z)
        sems = fwd_send.at[s, part], fwd_recv.at[s, part]
        return block_copy(part, source, core, *sems, {"ep": up_ep}, s == 0)

    def fwd_arrival(s, part):
        source = lax.rem(z - 1 - s + n_z, n_z)
        sems = fwd_send.at[s, part], fwd_recv.at[s, part]
        return block_copy(part, source, core, *sems, {"ep": up_ep})

    def bwd_copy(s, part):
        sems = bwd_send.at[s, part], bwd_recv.at[s, part]
        return block_copy(part, lax.rem(z + s, n_z), core, *sems, {"ep": down_ep}, s == 0)

    def bwd_arrival(s, part):
        sems = bwd_send.at[s, part], bwd_recv.at[s, part]
        return block_copy(part, lax.rem(z + 1 + s, n_z), core, *sems, {"ep": down_ep})

    def core_copy(k, part, source_z, source_core, mine=False):
        sems = core_send.at[k, part], core_recv.at[k, part]
        return block_copy(part, source_z, source_core, *sems, {"ep": other}, mine)

    def core_fwd(s, part, source_core):
        return core_copy(1 + s, part, lax.rem(z - 1 - s + n_z, n_z), source_core)

    def core_bwd(s, part, source_core):
        return core_copy(1 + reach + s, part, lax.rem(z + 1 + s, n_z), source_core)

    def fwd_sends(s):
        return jnp.logical_and(z - s >= 0, z + 1 <= n_z - 1)

    def fwd_gets(s):
        return z - 1 - s >= 0

    def bwd_sends(s):
        return lax.rem(z + s, n_z) <= reach - 2

    def bwd_gets(s):
        return lax.rem(z + 1 + s, n_z) <= reach - 2

    def bwd_needed(s):
        return jnp.logical_and(bwd_gets(s), lax.rem(z + 1 + s, n_z) < z)

    def back_copy(k, j):
        n = lax.rem(self_slot + far_first[k], here)
        q = lax.rem(t + j, n_tp)
        target = offset + n_tp * n
        away = jnp.logical_not(jnp.logical_and(target == me, q == t))
        return away, remote(
            result.at[q, n],
            back_ref.at[me],
            back_send.at[k, j],
            back_recv.at[me],
            {"ep": target, "tp": q},
        )

    token_rows = attended.shape[0] // n_tp

    def head_copy(k):
        q = lax.rem(t + k, n_tp)
        first = pl.multiple_of(q * token_rows, token_rows)
        return remote(
            attended.at[pl.ds(first, token_rows)],
            heads_ref.at[t],
            head_send.at[k],
            head_recv.at[k],
            {"tp": q},
        )

    width = result.shape[3]

    def expert_hidden(p):
        rows = rows_all[...].reshape(here * CAP, rows_all.shape[2])
        gate = dot(rows, gate_all[p])
        up = dot(rows, up_all[p])
        return (gate / (1.0 + jnp.exp(-gate)) * up).astype(BF16)

    def expert_part(p, first):
        hidden = expert_hidden(p)
        for q in range(n_tp):
            cols = slice(q * width, (q + 1) * width)
            piece = dot(hidden, down_all[p, :, cols]).astype(BF16).astype(F32)
            if first:
                total[:, cols] = piece
            else:
                total[:, cols] += piece

    def send_back(j):
        for k in range(here):
            away, copy = back_copy(k, j)

            @pl.when(away)
            def _(copy=copy):
                copy.start()

    def last_part(p):
        hidden = expert_hidden(p)
        for j in range(n_tp):
            q = lax.rem(t + j, n_tp)
            cols = pl.ds(pl.multiple_of(q * width, width), width)
            piece = dot(hidden, down_all[p, :, cols]).astype(BF16).astype(F32)
            done = (total[:, cols] + piece).astype(BF16)
            result[q] = done.reshape(here, CAP, width)
            if j > 0:
                send_back(j - 1)

        @pl.when(is_self)
        def _():
            back_ref[me] = result[t, self_slot]

        send_back(n_tp - 1)

    for a in range(3):
        for way in range(2):
            side_copy(a, way).start()

    key_ref[...] = row_norm(raw_key_ref[...], key_gain_ref[...]).astype(BF16)
    value_ref[...] = raw_value_ref[...].astype(F32).T.astype(BF16)
    keys_all[me] = key_ref[...]
    values_all[me] = value_ref[...]
    for copy in own:
        copy.start()
    own_out.start()
    for part in range(2):

        @pl.when(fwd_sends(0))
        def _(part=part):
            fwd_copy(0, part).start()

        @pl.when(bwd_sends(0))
        def _(part=part):
            bwd_copy(0, part).start()

        @pl.when(core == 0)
        def _(part=part):
            core_copy(0, part, z, 0, True).start()

    gather_rows(n_tp, offset, rows_ref, rows_gain_ref, routes_ref, send_ref, normed)
    columns_ref[...] = token_columns(routes_ref[...], route_weight_ref[...])
    for k in far_first:
        mate, copy = row_copy(k)

        @pl.when(mate != me)
        def _(copy=copy):
            copy.start()

    @pl.when(is_self)
    def _():
        rows_all[self_slot] = send_ref[self_slot]

    prepare_attention(
        heads, me + 1, query_ref, query_gain_ref, forget_ref, query_t, bias, run_max, run_sum, acc
    )
    for copy in own:
        copy.wait()

    hand_on(0)
    for s in range(reach):
        for part in range(2):

            @pl.when(fwd_gets(s))
            def _(s=s, part=part):
                fwd_arrival(s, part).wait_recv()

            if s + 1 < reach:

                @pl.when(fwd_sends(s + 1))
                def _(s=s, part=part):
                    fwd_copy(s + 1, part).start()

            @pl.when(fwd_gets(s))
            def _(s=s, part=part):
                core_fwd(s, part, core).start()

            if s < reach - 1:

                @pl.when(bwd_gets(s))
                def _(s=s, part=part):
                    bwd_arrival(s, part).wait_recv()

                if s + 1 < reach - 1:

                    @pl.when(bwd_sends(s + 1))
                    def _(s=s, part=part):
                        bwd_copy(s + 1, part).start()

                @pl.when(bwd_needed(s))
                def _(s=s, part=part):
                    core_bwd(s, part, core).start()

        if s == 0:
            hand_on(1)
        if s == 2:
            hand_on(2)
            for way in range(2):
                side_copy(3, way).start()
        if s == 3:
            for n in range(here):
                source, arrival = row_arrival(n)

                @pl.when(source != me)
                def _(arrival=arrival):
                    arrival.wait_recv()

            expert_part(t, True)
        if s == 4:
            expert_part(left, False)
        if s == 5:
            expert_part(right, False)
        if s == 6:
            for a in range(3):
                for way in range(2):
                    half_copy(a, way).wait_recv()
            last_part(across)

    hand_on(3)
    for part in range(2):

        @pl.when(core == 1)
        def _(part=part):
            core_copy(0, part, z, 0).wait_recv()

        for s in range(reach):

            @pl.when(fwd_gets(s))
            def _(s=s, part=part):
                core_fwd(s, part, 1 - core).wait_recv()

            if s < reach - 1:

                @pl.when(bwd_needed(s))
                def _(s=s, part=part):
                    core_bwd(s, part, 1 - core).wait_recv()

    state = (keys_all, values_all, query_t, bias, run_max, run_sum, acc)

    def body(block, carry):
        attend_block(block, False, *state)
        return carry

    for way in range(2):
        part_copy(way, out_first).start()
    lax.fori_loop(0, me, body, 0)
    attend_block(me, True, *state)
    finish_attention(heads, attended, run_sum, acc)
    for way in range(2):
        half_copy(3, way).wait_recv()
    part_copy(2, out_first).start()
    for k in range(1, n_tp):
        head_copy(k).start()
    own_first = pl.multiple_of(t * token_rows, token_rows)
    heads_ref[t] = attended[pl.ds(own_first, token_rows), :]
    slot = lax.broadcasted_iota(jnp.int32, (8, n_ep * CAP), 1).astype(F32)[:1]
    for j in range(TOP):
        picks[j] = jnp.where(columns_ref[:, j : j + 1] == slot, 1.0, 0.0).astype(BF16)

    for a in range(4):
        for way in range(2):
            side_copy(a, way).wait_send()
            half_copy(a, way).wait_send()
    for k in range(here):
        mate, copy = row_copy(k)

        @pl.when(mate != me)
        def _(copy=copy):
            copy.wait_send()

    for part in range(2):

        @pl.when(core == 0)
        def _(part=part):
            core_copy(0, part, z, 0, True).wait_send()

        for s in range(reach):

            @pl.when(fwd_sends(s))
            def _(s=s, part=part):
                fwd_copy(s, part).wait_send()

            @pl.when(fwd_gets(s))
            def _(s=s, part=part):
                core_fwd(s, part, core).wait_send()

            if s < reach - 1:

                @pl.when(bwd_sends(s))
                def _(s=s, part=part):
                    bwd_copy(s, part).wait_send()

                @pl.when(bwd_needed(s))
                def _(s=s, part=part):
                    core_bwd(s, part, core).wait_send()

    for k in range(3):
        part_copy(k, out_first).wait_send()
        part_copy(k, (1 - core) * out_rows).wait_recv()
    own_out.wait()
    for k in range(1, n_tp):
        source = lax.rem(t + n_tp - k, n_tp)
        head_copy(k).wait_send()
        remote(
            attended.at[pl.ds(0, token_rows)],
            heads_ref.at[source],
            head_send.at[k],
            head_recv.at[k],
            {"tp": source},
        ).wait_recv()
    projected = None
    for k in range(n_tp):
        piece = dot(heads_ref[k], out_all[k])
        projected = piece if projected is None else projected + piece
    mixer_ref[...] = projected.astype(BF16)

    for k in range(here):
        for j in range(n_tp):
            away, copy = back_copy(k, j)

            @pl.when(away)
            def _(copy=copy):
                copy.wait_send()

    for e in range(n_ep):
        column, away = returns_from(e)
        arrival = remote(
            result.at[0, 0],
            back_ref.at[e],
            back_send.at[0, 0],
            back_recv.at[e],
            {"ep": e, "tp": column},
        )

        @pl.when(away)
        def _(arrival=arrival):
            arrival.wait_recv()

    expert_out = None
    for j in range(TOP):
        picked = dot(picks[j], back_ref[...].reshape(n_ep * CAP, back_ref.shape[2]))
        term = picked * columns_ref[:, TOP + j : TOP + j + 1]
        expert_out = term if expert_out is None else expert_out + term
    expert_ref[...] = expert_out.astype(BF16)


def settle_kernel(mixer_in, expert_in, mixer_ref, expert_ref):
    mixer_ref[...] = mixer_in[...]
    expert_ref[...] = expert_in[...]


def on_device(
    n_ep,
    n_tp,
    queries,
    key_rows,
    value_rows,
    query_gain,
    key_gain,
    log_forget,
    out_weight,
    expert_rows,
    expert_gain,
    routes,
    route_weight,
    gate_weight,
    up_weight,
    down_weight,
):
    span, model_width = expert_rows.shape
    here = n_ep // n_tp
    heads = queries.shape[1] // HEAD_SIZE
    width = model_width // n_tp
    n_z = n_ep // CORES
    reach = n_z // 2
    ff_part = gate_weight.shape[2]
    hbm = pl.BlockSpec(memory_space=pltpu.HBM)
    vmem = pl.BlockSpec(memory_space=pltpu.VMEM)
    shape = jax.ShapeDtypeStruct
    dma = pltpu.SemaphoreType.DMA
    columns = heads * span
    mixer_out, expert_out = pl.pallas_call(
        functools.partial(layer_kernel, n_ep, n_tp, heads),
        out_shape=(
            shape((span // n_tp, model_width), BF16),
            shape((span, width), BF16),
        ),
        in_specs=[vmem] * 10 + [hbm] * 4,
        out_specs=(vmem, vmem),
        scratch_shapes=[
            pltpu.VMEM((here, CAP, model_width), BF16),
            pltpu.VMEM((span, model_width), BF16),
            pltpu.VMEM((span, 8), F32),
            pltpu.VMEM((TOP, span, n_ep * CAP), BF16),
            pltpu.VMEM((n_ep, CAP, width), BF16),
            pltpu.VMEM((n_tp, span // n_tp, heads * HEAD_SIZE), BF16),
            pltpu.VMEM((n_tp, *out_weight.shape), BF16),
            pltpu.VMEM((span, HEAD_SIZE), BF16),
            pltpu.VMEM((HEAD_SIZE, span), BF16),
            pltpu.VMEM((here, CAP, model_width), BF16),
            pltpu.VMEM((here * CAP, model_width), F32),
            pltpu.VMEM((n_tp, here, CAP, width), BF16),
            pltpu.VMEM((span, heads * HEAD_SIZE), BF16),
            pltpu.VMEM((n_ep, span, HEAD_SIZE), BF16),
            pltpu.VMEM((n_ep, HEAD_SIZE, span), BF16),
            pltpu.VMEM((2 * HEAD_SIZE, columns), BF16),
            pltpu.VMEM((n_ep, span, HEAD_SIZE), BF16),
            pltpu.VMEM((1, columns), F32),
            pltpu.VMEM((1, columns), F32),
            pltpu.VMEM((HEAD_SIZE, columns), F32),
            pltpu.VMEM((n_tp, model_width, ff_part), BF16),
            pltpu.VMEM((n_tp, model_width, ff_part), BF16),
            pltpu.VMEM((n_tp, ff_part, model_width), BF16),
            dma((here,)),
            dma((here,)),
            dma((reach, 2)),
            dma((reach, 2)),
            dma((reach - 1, 2)),
            dma((reach - 1, 2)),
            dma((2 * reach, 2)),
            dma((2 * reach, 2)),
            dma((4, 2)),
            dma((4, 2)),
            dma((4, 2)),
            dma((4, 2)),
            dma((3,)),
            dma((3,)),
            dma((here, n_tp)),
            dma((n_ep,)),
            dma((n_tp,)),
            dma((n_tp,)),
            dma((4,)),
        ],
        compiler_params=pltpu.CompilerParams(
            collective_id=0, has_side_effects=True, vmem_limit_bytes=60 * 1024 * 1024
        ),
        name="layer",
    )(
        expert_rows,
        expert_gain.reshape(1, -1),
        routes,
        route_weight,
        key_rows,
        value_rows,
        key_gain.reshape(1, -1),
        queries,
        query_gain.reshape(1, -1),
        log_forget,
        gate_weight.reshape(model_width, ff_part),
        up_weight.reshape(model_width, ff_part),
        down_weight.reshape(ff_part, model_width),
        out_weight,
    )
    steps = 2
    mixer_block = pl.BlockSpec((span // n_tp // steps, model_width), lambda i: (i, 0))
    expert_block = pl.BlockSpec((span // steps, width), lambda i: (i, 0))
    return pl.pallas_call(
        settle_kernel,
        grid=(steps,),
        out_shape=(
            shape((span // n_tp, model_width), BF16),
            shape((span, width), BF16),
        ),
        in_specs=[mixer_block, expert_block],
        out_specs=(mixer_block, expert_block),
        name="settle",
    )(mixer_out, expert_out)


def solution(mesh):
    in_specs = (
        P(("grp", "ep"), "tp"),
        P(("grp", "ep"), "tp"),
        P(("grp", "ep"), "tp"),
        P(),
        P(),
        P("tp", "grp"),
        P("tp", None),
        P(("grp", "ep"), None),
        P(),
        P(None, ("grp", "ep")),
        P(None, ("grp", "ep")),
        P("ep", None, "tp"),
        P("ep", None, "tp"),
        P("ep", "tp", None),
    )
    out_specs = (P(("grp", "ep", "tp"), None), P(("grp", "ep"), "tp"))
    return jax.shard_map(
        functools.partial(on_device, mesh.shape["ep"], mesh.shape["tp"]),
        mesh=mesh,
        in_specs=in_specs,
        out_specs=out_specs,
        check_vma=False,
    )
```

```python
import functools

import jax
import jax.numpy as jnp
from jax import lax
from jax.experimental import pallas as pl
from jax.experimental.pallas import tpu as pltpu
from jax.sharding import PartitionSpec as P

HEAD_SIZE = 128
EXPERTS = 32
CAP = 48
TOP = 2
CORES = 2
LOG2E = 1.4426950408889634
MESH = pl.DeviceIdType.MESH
F32 = jnp.float32
BF16 = jnp.bfloat16


def dot(a, b, dims=(((1,), (0,)), ((), ()))):
    return lax.dot_general(a, b, dims, preferred_element_type=F32)


def row_norm(rows, gain):
    wide = rows.astype(F32)
    factor = lax.rsqrt(jnp.mean(wide * wide, axis=-1, keepdims=True) + 1e-06)
    return wide * factor * gain


def member_and_rank(routes, expert_col):
    tokens = routes.shape[1]
    named = jnp.logical_or(routes[0:1, :] == expert_col, routes[1:2, :] == expert_col)
    member = jnp.where(named, 1.0, 0.0).astype(F32)
    before = lax.broadcasted_iota(jnp.int32, (tokens, tokens), 0)
    after = lax.broadcasted_iota(jnp.int32, (tokens, tokens), 1)
    earlier = jnp.where(before < after, 1.0, 0.0).astype(BF16)
    return member, dot(member.astype(BF16), earlier)


def gather_rows(n_tp, offset, rows_ref, gain_ref, routes_ref, send, normed):
    span = rows_ref.shape[0]
    step = 64
    for first in range(0, span, step):
        normed[first : first + step, :] = row_norm(
            rows_ref[first : first + step, :], gain_ref[...]
        ).astype(BF16)
    here = EXPERTS // n_tp
    expert_col = offset + n_tp * lax.broadcasted_iota(jnp.int32, (here, 1), 0)
    member, rank = member_and_rank(routes_ref[...], expert_col)
    place = jnp.where(member > 0.5, rank, -1.0)
    slot = lax.broadcasted_iota(jnp.int32, (CAP, span), 0).astype(F32)
    for m in range(here):
        pick = jnp.where(place[m : m + 1, :] == slot, 1.0, 0.0).astype(BF16)
        send[m] = dot(pick, normed[...]).astype(BF16)


def token_columns(routes, weights):
    expert_col = lax.broadcasted_iota(jnp.int32, (EXPERTS, 1), 0)
    _, rank = member_and_rank(routes, expert_col)
    rows = []
    for j in range(TOP):
        chosen = routes[j : j + 1, :]
        within = jnp.sum(jnp.where(chosen == expert_col, rank, 0.0), axis=0, keepdims=True)
        rows.append((chosen * CAP).astype(F32) + within)
    rows.append(weights)
    rows.append(jnp.zeros((8 - 2 * TOP, routes.shape[1]), F32))
    return jnp.concatenate(rows, axis=0).T


def split_three(value):
    high = value.astype(BF16)
    rest = value - high.astype(F32)
    mid = rest.astype(BF16)
    low = (rest - mid.astype(F32)).astype(BF16)
    return high.astype(F32), mid.astype(F32), low.astype(F32)


def prepare_attention(
    heads, blocks, query_ref, gain_ref, forget_ref, query_t, bias, run_max, run_sum, acc
):
    span = query_ref.shape[0]
    columns = heads * span
    for h in range(heads):
        normed = row_norm(query_ref[:, h * HEAD_SIZE : (h + 1) * HEAD_SIZE], gain_ref[...])
        rounded = normed.astype(BF16).astype(F32)
        query_t[:HEAD_SIZE, h * span : (h + 1) * span] = rounded.T.astype(BF16)
    row = lax.broadcasted_iota(jnp.int32, (HEAD_SIZE, columns), 0)
    head = lax.broadcasted_iota(jnp.int32, (HEAD_SIZE, columns), 1) // span
    query_t[HEAD_SIZE:, :] = jnp.where(row // 3 == head, 1.0, 0.0).astype(BF16)
    run_max[...] = jnp.full(run_max.shape, -1e30, F32)
    run_sum[...] = jnp.zeros(run_sum.shape, F32)
    acc[...] = jnp.zeros(acc.shape, F32)
    lane = lax.broadcasted_iota(jnp.int32, (8, HEAD_SIZE), 1)
    sub = lax.broadcasted_iota(jnp.int32, (8, HEAD_SIZE), 0)
    place = jnp.where(lane == sub, 1.0, 0.0).astype(BF16)

    def one(block, carry):
        first = pl.multiple_of(block * span, span)
        rows = []
        for h in range(heads):
            gates = forget_ref[h : h + 1, pl.ds(first, span)]
            rows.extend(split_three(gates * (-(HEAD_SIZE**0.5))))
        rows.append(jnp.zeros((8 - len(rows), span), F32))
        stacked = jnp.concatenate(rows, axis=0).astype(BF16)
        bias[block] = dot(stacked, place, (((0,), (0,)), ((), ()))).astype(BF16)
        return carry

    lax.fori_loop(0, blocks, one, 0)


def attend_block(block, masked, keys_all, values_all, query_t, bias, run_max, run_sum, acc):
    span = keys_all.shape[1]
    columns = query_t.shape[1]
    exp_scale = HEAD_SIZE ** (-0.5) * LOG2E
    width = 256
    keys = jnp.concatenate([keys_all[block], bias[block]], axis=1)
    values = values_all[block]
    for first_col in range(0, columns, width):
        cols = slice(first_col, first_col + width)
        scores = dot(keys, query_t[:, cols])
        if masked:
            key_at = lax.broadcasted_iota(jnp.int32, (span, width), 0)
            query_at = lax.broadcasted_iota(jnp.int32, (span, width), 1) + first_col % span
            scores = jnp.where(key_at <= query_at, scores, -1e30)
        old_max = run_max[:, cols]
        new_max = jnp.maximum(old_max, jnp.max(scores, axis=0, keepdims=True))
        shrink = jnp.exp2((old_max - new_max) * exp_scale)
        weights = jnp.exp2((scores - new_max) * exp_scale)
        run_max[:, cols] = new_max
        run_sum[:, cols] = shrink * run_sum[:, cols] + jnp.sum(weights, axis=0, keepdims=True)
        acc[:, cols] = shrink * acc[:, cols] + dot(values, weights.astype(BF16))


def finish_attention(heads, out_ref, run_sum, acc):
    span = out_ref.shape[0]
    for h in range(heads):
        cols = slice(h * span, (h + 1) * span)
        attended = (acc[:, cols] / run_sum[:, cols]).T
        out_ref[:, h * HEAD_SIZE : (h + 1) * HEAD_SIZE] = attended.astype(BF16)


def remote(src, dst, send_sem, recv_sem, where):
    return pltpu.make_async_remote_copy(
        src_ref=src,
        dst_ref=dst,
        send_sem=send_sem,
        recv_sem=recv_sem,
        device_id=where,
        device_id_type=MESH,
    )


def layer_kernel(
    n_ep,
    n_tp,
    heads,
    rows_ref,
    rows_gain_ref,
    routes_ref,
    route_weight_ref,
    raw_key_ref,
    raw_value_ref,
    key_gain_ref,
    query_ref,
    query_gain_ref,
    forget_ref,
    gate_ref,
    up_ref,
    down_ref,
    out_ref,
    mixer_ref,
    expert_ref,
    send_ref,
    normed,
    columns_ref,
    picks,
    back_ref,
    heads_ref,
    out_all,
    key_ref,
    value_ref,
    rows_all,
    total,
    result,
    attended,
    keys_all,
    values_all,
    query_t,
    bias,
    run_max,
    run_sum,
    acc,
    gate_all,
    up_all,
    down_all,
    row_send,
    row_recv,
    fwd_send,
    fwd_recv,
    bwd_send,
    bwd_recv,
    core_send,
    core_recv,
    side_send,
    side_recv,
    half_send,
    half_recv,
    part_send,
    part_recv,
    back_send,
    back_recv,
    head_send,
    head_recv,
    local,
):
    me, t = lax.axis_index("ep"), lax.axis_index("tp")
    n_z = n_ep // CORES
    z, core = me // CORES, lax.rem(me, CORES)
    offset = lax.rem(t + (n_tp - 1) * me, n_tp)
    here = n_ep // n_tp
    right, left = lax.rem(t + 1, n_tp), lax.rem(t + n_tp - 1, n_tp)
    across = lax.rem(t + 2, n_tp)
    up_ep = CORES * lax.rem(z + 1, n_z) + core
    down_ep = CORES * lax.rem(z + n_z - 1, n_z) + core
    other = CORES * z + (1 - core)
    reach = n_z // 2
    self_slot = me // n_tp
    is_self = lax.rem(me, n_tp) == offset
    far_first = [here // 2]
    for k in range(1, here // 2):
        far_first += [here // 2 - k, here // 2 + k]
    far_first.append(0)

    barrier = pltpu.get_barrier_semaphore()
    for where in (
        {"ep": up_ep},
        {"ep": down_ep},
        {"ep": other},
        {"tp": right},
        {"tp": left},
        {"tp": across},
    ):
        pl.semaphore_signal(barrier, inc=1, device_id=where, device_id_type=MESH)
    for m in range(here):
        mate = offset + n_tp * m

        @pl.when(mate != me)
        def _(mate=mate):
            pl.semaphore_signal(barrier, inc=1, device_id={"ep": mate}, device_id_type=MESH)

    def returns_from(e):
        column = lax.rem(me + e, n_tp)
        return column, jnp.logical_not(jnp.logical_and(me == e, column == t))

    for e in range(n_ep):
        column, away = returns_from(e)

        @pl.when(away)
        def _(e=e, column=column):
            pl.semaphore_signal(
                barrier, inc=1, device_id={"ep": e, "tp": column}, device_id_type=MESH
            )

    pl.semaphore_wait(barrier, 6 + here + n_ep - jnp.where(is_self, 2, 0))

    weights = ((gate_ref, gate_all), (up_ref, up_all), (down_ref, down_all))
    out_rows = out_ref.shape[0] // CORES
    out_first = core * out_rows

    def side_copy(a, way):
        where = {"tp": (right, left)[way]}
        if a < 3:
            src, dst = weights[a][0], weights[a][1].at[t]
        else:
            mine = pl.ds(out_first, out_rows)
            src, dst = out_ref.at[mine], out_all.at[t, mine]
        return remote(src, dst, side_send.at[a, way], side_recv.at[a, way], where)

    def half_copy(a, way):
        where = {"tp": (right, left)[way]}
        owner = (left, right)[way]
        if a < 3:
            full = weights[a][1]
            half = full.shape[1] // 2
            part = full.at[owner, pl.ds(way * half, half)]
        else:
            half = out_rows // 2
            part = out_all.at[owner, pl.ds(out_first + way * half, half)]
        return remote(part, part, half_send.at[a, way], half_recv.at[a, way], where)

    def hand_on(a):
        for way in range(2):
            side_copy(a, way).wait_recv()
            half_copy(a, way).start()

    def part_copy(k, first):
        part = out_all.at[(left, right, across)[k], pl.ds(first, out_rows)]
        return remote(part, part, part_send.at[k], part_recv.at[k], {"ep": other})

    own = [
        pltpu.make_async_copy(src, full.at[t], local.at[a])
        for a, (src, full) in enumerate(weights)
    ]
    own_out = pltpu.make_async_copy(out_ref, out_all.at[t], local.at[3])

    def row_copy(k):
        m = lax.rem(self_slot + k, here)
        mate = offset + n_tp * m
        return mate, remote(
            send_ref.at[m],
            rows_all.at[self_slot],
            row_send.at[m],
            row_recv.at[self_slot],
            {"ep": mate},
        )

    def row_arrival(n):
        source = offset + n_tp * n
        return source, remote(
            send_ref.at[n], rows_all.at[n], row_send.at[n], row_recv.at[n], {"ep": source}
        )

    def block_copy(part, source_z, source_core, send_sem, recv_sem, where, mine=False):
        block = (keys_all, values_all)[part].at[CORES * source_z + source_core]
        return remote((key_ref, value_ref)[part] if mine else block, block, send_sem, recv_sem, where)

    def fwd_copy(s, part):
        source = lax.rem(z - s + n_z, n_z)
        sems = fwd_send.at[s, part], fwd_recv.at[s, part]
        return block_copy(part, source, core, *sems, {"ep": up_ep}, s == 0)

    def fwd_arrival(s, part):
        source = lax.rem(z - 1 - s + n_z, n_z)
        sems = fwd_send.at[s, part], fwd_recv.at[s, part]
        return block_copy(part, source, core, *sems, {"ep": up_ep})

    def bwd_copy(s, part):
        sems = bwd_send.at[s, part], bwd_recv.at[s, part]
        return block_copy(part, lax.rem(z + s, n_z), core, *sems, {"ep": down_ep}, s == 0)

    def bwd_arrival(s, part):
        sems = bwd_send.at[s, part], bwd_recv.at[s, part]
        return block_copy(part, lax.rem(z + 1 + s, n_z), core, *sems, {"ep": down_ep})

    def core_copy(k, part, source_z, source_core, mine=False):
        sems = core_send.at[k, part], core_recv.at[k, part]
        return block_copy(part, source_z, source_core, *sems, {"ep": other}, mine)

    def core_fwd(s, part, source_core):
        return core_copy(1 + s, part, lax.rem(z - 1 - s + n_z, n_z), source_core)

    def core_bwd(s, part, source_core):
        return core_copy(1 + reach + s, part, lax.rem(z + 1 + s, n_z), source_core)

    def fwd_sends(s):
        return jnp.logical_and(z - s >= 0, z + 1 <= n_z - 1)

    def fwd_gets(s):
        return z - 1 - s >= 0

    def bwd_sends(s):
        return lax.rem(z + s, n_z) <= reach - 2

    def bwd_gets(s):
        return lax.rem(z + 1 + s, n_z) <= reach - 2

    def bwd_needed(s):
        return jnp.logical_and(bwd_gets(s), lax.rem(z + 1 + s, n_z) < z)

    def back_copy(k, j):
        n = lax.rem(self_slot + far_first[k], here)
        q = lax.rem(t + j, n_tp)
        target = offset + n_tp * n
        away = jnp.logical_not(jnp.logical_and(target == me, q == t))
        return away, remote(
            result.at[q, n],
            back_ref.at[me],
            back_send.at[k, j],
            back_recv.at[me],
            {"ep": target, "tp": q},
        )

    token_rows = attended.shape[0] // n_tp

    def head_copy(k):
        q = lax.rem(t + k, n_tp)
        first = pl.multiple_of(q * token_rows, token_rows)
        return remote(
            attended.at[pl.ds(first, token_rows)],
            heads_ref.at[t],
            head_send.at[k],
            head_recv.at[k],
            {"tp": q},
        )

    def expert_part(p, first):
        rows = rows_all[...].reshape(here * CAP, rows_all.shape[2])
        gate = dot(rows, gate_all[p])
        up = dot(rows, up_all[p])
        hidden = (gate / (1.0 + jnp.exp(-gate)) * up).astype(BF16)
        width = result.shape[3]
        for q in range(n_tp):
            cols = slice(q * width, (q + 1) * width)
            piece = dot(hidden, down_all[p, :, cols]).astype(BF16).astype(F32)
            if first:
                total[:, cols] = piece
            else:
                total[:, cols] += piece

    for a in range(3):
        for way in range(2):
            side_copy(a, way).start()

    key_ref[...] = row_norm(raw_key_ref[...], key_gain_ref[...]).astype(BF16)
    value_ref[...] = raw_value_ref[...].astype(F32).T.astype(BF16)
    keys_all[me] = key_ref[...]
    values_all[me] = value_ref[...]
    for copy in own:
        copy.start()
    own_out.start()
    for part in range(2):

        @pl.when(fwd_sends(0))
        def _(part=part):
            fwd_copy(0, part).start()

        @pl.when(bwd_sends(0))
        def _(part=part):
            bwd_copy(0, part).start()

        @pl.when(core == 0)
        def _(part=part):
            core_copy(0, part, z, 0, True).start()

    gather_rows(n_tp, offset, rows_ref, rows_gain_ref, routes_ref, send_ref, normed)
    columns_ref[...] = token_columns(routes_ref[...], route_weight_ref[...])
    for k in far_first:
        mate, copy = row_copy(k)

        @pl.when(mate != me)
        def _(copy=copy):
            copy.start()

    @pl.when(is_self)
    def _():
        rows_all[self_slot] = send_ref[self_slot]

    prepare_attention(
        heads, me + 1, query_ref, query_gain_ref, forget_ref, query_t, bias, run_max, run_sum, acc
    )
    for copy in own:
        copy.wait()

    hand_on(0)
    for s in range(reach):
        for part in range(2):

            @pl.when(fwd_gets(s))
            def _(s=s, part=part):
                fwd_arrival(s, part).wait_recv()

            if s + 1 < reach:

                @pl.when(fwd_sends(s + 1))
                def _(s=s, part=part):
                    fwd_copy(s + 1, part).start()

            @pl.when(fwd_gets(s))
            def _(s=s, part=part):
                core_fwd(s, part, core).start()

            if s < reach - 1:

                @pl.when(bwd_gets(s))
                def _(s=s, part=part):
                    bwd_arrival(s, part).wait_recv()

                if s + 1 < reach - 1:

                    @pl.when(bwd_sends(s + 1))
                    def _(s=s, part=part):
                        bwd_copy(s + 1, part).start()

                @pl.when(bwd_needed(s))
                def _(s=s, part=part):
                    core_bwd(s, part, core).start()

        if s == 0:
            hand_on(1)
        if s == 2:
            hand_on(2)
            for way in range(2):
                side_copy(3, way).start()
        if s == 3:
            for n in range(here):
                source, arrival = row_arrival(n)

                @pl.when(source != me)
                def _(arrival=arrival):
                    arrival.wait_recv()

            expert_part(t, True)
        if s == 4:
            expert_part(left, False)
        if s == 5:
            expert_part(right, False)
        if s == 6:
            for a in range(3):
                for way in range(2):
                    half_copy(a, way).wait_recv()
            expert_part(across, False)
            width = result.shape[3]
            for k in far_first:
                n = lax.rem(self_slot + k, here)
                first = pl.multiple_of(n * CAP, CAP)
                for q in range(n_tp):
                    result[q, n] = total[pl.ds(first, CAP), q * width : (q + 1) * width].astype(
                        BF16
                    )
            for k in range(here):
                for j in range(n_tp):
                    away, copy = back_copy(k, j)

                    @pl.when(away)
                    def _(copy=copy):
                        copy.start()

            @pl.when(is_self)
            def _():
                back_ref[me] = result[t, self_slot]

    hand_on(3)
    for part in range(2):

        @pl.when(core == 1)
        def _(part=part):
            core_copy(0, part, z, 0).wait_recv()

        for s in range(reach):

            @pl.when(fwd_gets(s))
            def _(s=s, part=part):
                core_fwd(s, part, 1 - core).wait_recv()

            if s < reach - 1:

                @pl.when(bwd_needed(s))
                def _(s=s, part=part):
                    core_bwd(s, part, 1 - core).wait_recv()

    state = (keys_all, values_all, query_t, bias, run_max, run_sum, acc)

    def body(block, carry):
        attend_block(block, False, *state)
        return carry

    for way in range(2):
        part_copy(way, out_first).start()
    lax.fori_loop(0, me, body, 0)
    attend_block(me, True, *state)
    finish_attention(heads, attended, run_sum, acc)
    for way in range(2):
        half_copy(3, way).wait_recv()
    part_copy(2, out_first).start()
    for k in range(1, n_tp):
        head_copy(k).start()
    own_first = pl.multiple_of(t * token_rows, token_rows)
    heads_ref[t] = attended[pl.ds(own_first, token_rows), :]
    slot = lax.broadcasted_iota(jnp.int32, (8, n_ep * CAP), 1).astype(F32)[:1]
    for j in range(TOP):
        picks[j] = jnp.where(columns_ref[:, j : j + 1] == slot, 1.0, 0.0).astype(BF16)

    for a in range(4):
        for way in range(2):
            side_copy(a, way).wait_send()
            half_copy(a, way).wait_send()
    for k in range(here):
        mate, copy = row_copy(k)

        @pl.when(mate != me)
        def _(copy=copy):
            copy.wait_send()

    for part in range(2):

        @pl.when(core == 0)
        def _(part=part):
            core_copy(0, part, z, 0, True).wait_send()

        for s in range(reach):

            @pl.when(fwd_sends(s))
            def _(s=s, part=part):
                fwd_copy(s, part).wait_send()

            @pl.when(fwd_gets(s))
            def _(s=s, part=part):
                core_fwd(s, part, core).wait_send()

            if s < reach - 1:

                @pl.when(bwd_sends(s))
                def _(s=s, part=part):
                    bwd_copy(s, part).wait_send()

                @pl.when(bwd_needed(s))
                def _(s=s, part=part):
                    core_bwd(s, part, core).wait_send()

    for k in range(3):
        part_copy(k, out_first).wait_send()
        part_copy(k, (1 - core) * out_rows).wait_recv()
    own_out.wait()
    for k in range(1, n_tp):
        source = lax.rem(t + n_tp - k, n_tp)
        head_copy(k).wait_send()
        remote(
            attended.at[pl.ds(0, token_rows)],
            heads_ref.at[source],
            head_send.at[k],
            head_recv.at[k],
            {"tp": source},
        ).wait_recv()
    projected = None
    for k in range(n_tp):
        piece = dot(heads_ref[k], out_all[k])
        projected = piece if projected is None else projected + piece
    mixer_ref[...] = projected.astype(BF16)

    for k in range(here):
        for j in range(n_tp):
            away, copy = back_copy(k, j)

            @pl.when(away)
            def _(copy=copy):
                copy.wait_send()

    for e in range(n_ep):
        column, away = returns_from(e)
        arrival = remote(
            result.at[0, 0],
            back_ref.at[e],
            back_send.at[0, 0],
            back_recv.at[e],
            {"ep": e, "tp": column},
        )

        @pl.when(away)
        def _(arrival=arrival):
            arrival.wait_recv()

    expert_out = None
    for j in range(TOP):
        picked = dot(picks[j], back_ref[...].reshape(n_ep * CAP, back_ref.shape[2]))
        term = picked * columns_ref[:, TOP + j : TOP + j + 1]
        expert_out = term if expert_out is None else expert_out + term
    expert_ref[...] = expert_out.astype(BF16)


def settle_kernel(mixer_in, expert_in, mixer_ref, expert_ref):
    mixer_ref[...] = mixer_in[...]
    expert_ref[...] = expert_in[...]


def on_device(
    n_ep,
    n_tp,
    queries,
    key_rows,
    value_rows,
    query_gain,
    key_gain,
    log_forget,
    out_weight,
    expert_rows,
    expert_gain,
    routes,
    route_weight,
    gate_weight,
    up_weight,
    down_weight,
):
    span, model_width = expert_rows.shape
    here = n_ep // n_tp
    heads = queries.shape[1] // HEAD_SIZE
    width = model_width // n_tp
    n_z = n_ep // CORES
    reach = n_z // 2
    ff_part = gate_weight.shape[2]
    hbm = pl.BlockSpec(memory_space=pltpu.HBM)
    vmem = pl.BlockSpec(memory_space=pltpu.VMEM)
    shape = jax.ShapeDtypeStruct
    dma = pltpu.SemaphoreType.DMA
    columns = heads * span
    mixer_out, expert_out = pl.pallas_call(
        functools.partial(layer_kernel, n_ep, n_tp, heads),
        out_shape=(
            shape((span // n_tp, model_width), BF16),
            shape((span, width), BF16),
        ),
        in_specs=[vmem] * 10 + [hbm] * 4,
        out_specs=(vmem, vmem),
        scratch_shapes=[
            pltpu.VMEM((here, CAP, model_width), BF16),
            pltpu.VMEM((span, model_width), BF16),
            pltpu.VMEM((span, 8), F32),
            pltpu.VMEM((TOP, span, n_ep * CAP), BF16),
            pltpu.VMEM((n_ep, CAP, width), BF16),
            pltpu.VMEM((n_tp, span // n_tp, heads * HEAD_SIZE), BF16),
            pltpu.VMEM((n_tp, *out_weight.shape), BF16),
            pltpu.VMEM((span, HEAD_SIZE), BF16),
            pltpu.VMEM((HEAD_SIZE, span), BF16),
            pltpu.VMEM((here, CAP, model_width), BF16),
            pltpu.VMEM((here * CAP, model_width), F32),
            pltpu.VMEM((n_tp, here, CAP, width), BF16),
            pltpu.VMEM((span, heads * HEAD_SIZE), BF16),
            pltpu.VMEM((n_ep, span, HEAD_SIZE), BF16),
            pltpu.VMEM((n_ep, HEAD_SIZE, span), BF16),
            pltpu.VMEM((2 * HEAD_SIZE, columns), BF16),
            pltpu.VMEM((n_ep, span, HEAD_SIZE), BF16),
            pltpu.VMEM((1, columns), F32),
            pltpu.VMEM((1, columns), F32),
            pltpu.VMEM((HEAD_SIZE, columns), F32),
            pltpu.VMEM((n_tp, model_width, ff_part), BF16),
            pltpu.VMEM((n_tp, model_width, ff_part), BF16),
            pltpu.VMEM((n_tp, ff_part, model_width), BF16),
            dma((here,)),
            dma((here,)),
            dma((reach, 2)),
            dma((reach, 2)),
            dma((reach - 1, 2)),
            dma((reach - 1, 2)),
            dma((2 * reach, 2)),
            dma((2 * reach, 2)),
            dma((4, 2)),
            dma((4, 2)),
            dma((4, 2)),
            dma((4, 2)),
            dma((3,)),
            dma((3,)),
            dma((here, n_tp)),
            dma((n_ep,)),
            dma((n_tp,)),
            dma((n_tp,)),
            dma((4,)),
        ],
        compiler_params=pltpu.CompilerParams(
            collective_id=0, has_side_effects=True, vmem_limit_bytes=60 * 1024 * 1024
        ),
        name="layer",
    )(
        expert_rows,
        expert_gain.reshape(1, -1),
        routes,
        route_weight,
        key_rows,
        value_rows,
        key_gain.reshape(1, -1),
        queries,
        query_gain.reshape(1, -1),
        log_forget,
        gate_weight.reshape(model_width, ff_part),
        up_weight.reshape(model_width, ff_part),
        down_weight.reshape(ff_part, model_width),
        out_weight,
    )
    steps = 2
    mixer_block = pl.BlockSpec((span // n_tp // steps, model_width), lambda i: (i, 0))
    expert_block = pl.BlockSpec((span // steps, width), lambda i: (i, 0))
    return pl.pallas_call(
        settle_kernel,
        grid=(steps,),
        out_shape=(
            shape((span // n_tp, model_width), BF16),
            shape((span, width), BF16),
        ),
        in_specs=[mixer_block, expert_block],
        out_specs=(mixer_block, expert_block),
        name="settle",
    )(mixer_out, expert_out)


def solution(mesh):
    in_specs = (
        P(("grp", "ep"), "tp"),
        P(("grp", "ep"), "tp"),
        P(("grp", "ep"), "tp"),
        P(),
        P(),
        P("tp", "grp"),
        P("tp", None),
        P(("grp", "ep"), None),
        P(),
        P(None, ("grp", "ep")),
        P(None, ("grp", "ep")),
        P("ep", None, "tp"),
        P("ep", None, "tp"),
        P("ep", "tp", None),
    )
    out_specs = (P(("grp", "ep", "tp"), None), P(("grp", "ep"), "tp"))
    return jax.shard_map(
        functools.partial(on_device, mesh.shape["ep"], mesh.shape["tp"]),
        mesh=mesh,
        in_specs=in_specs,
        out_specs=out_specs,
        check_vma=False,
    )
```
